128 devices in a mesh: ep: 64 (over z, y, x), tp: 2 (over core).
Axes of the slice: x: 4, y: 4, z: 4, core: 2. Of those that a mesh axis runs over, the one named last changes fastest.
Arguments:
- tokens: bfloat16 [24576, 3072], P('ep', 'tp'), may hold values from -6 to 6
- cotangent: bfloat16 [24576, 3072], P('ep', 'tp'), may hold values from -6 to 6
- experts: int32 [24576, 2], P('ep'), may hold values from 0 to 63, all different within a row; in each aligned block of 384 rows (0 to 383, 384 to 767, ...) at most 18 rows name the same one
- gate: float32 [24576, 2], P('ep'), may hold values from 0.2 to 1
- w_gate: bfloat16 [64, 3072, 768], P('ep', None, 'tp'), may hold values from -0.109375 to 0.109375
- w_up: bfloat16 [64, 3072, 768], P('ep', None, 'tp'), may hold values from -0.109375 to 0.109375
- w_down: bfloat16 [64, 768, 3072], P('ep', 'tp'), may hold values from -0.21875 to 0.21875
Outputs:
- token_grad: bfloat16 [24576, 3072], P('ep', 'tp')
- gate_grad: float32 [24576, 2], P('ep')
- gate_weight_grad: bfloat16 [64, 3072, 768], P('ep', None, 'tp')
- up_weight_grad: bfloat16 [64, 3072, 768], P('ep', None, 'tp')
- down_weight_grad: bfloat16 [64, 768, 3072], P('ep', 'tp')
- gate_row_norms: float32 [64, 3072], P('ep')
- up_row_norms: float32 [64, 3072], P('ep')
- down_row_norms: float32 [64, 768], P('ep', 'tp')
The draws below stay inside these ranges and needn't reach their ends.
Inputs may be any that keep to these rules, and one draw needn't show every extreme that they name: A row names 2 different experts. In each aligned block of 384 rows (the rows of one index of ep) no expert is named by more than 18 rows, a bound that some block reaches.
All inputs are finite; a program needn't handle non-finite values.
Results may differ from the reference program's by a relative error of at most 0.008.
Values may be sent and summed in bfloat16 or wider, within the bound.
No kernel may reach another device: no remote copies, remote signals or barrier semaphores. Data moves between devices by JAX's collectives and lax.ppermute only.
A program may use at most 128 MiB of HBM per device.

```python
import math
import jax
import jax.numpy as jnp
import numpy as np
from jax import lax

D = 3072
F = 768
TOP = 2
TOK_EP = 384
EXPERTS = 64
CAP = 18
TOKENS = 24576
N_EP = 64
N_TP = 2


def shard_levels(own_key, extent, cuts, low, high):
    def one(position, blocks):
        steps = jax.random.uniform(jax.random.fold_in(jax.random.fold_in(own_key, 6), position), (blocks,), jnp.float32, low / len(cuts), high / len(cuts))
        return jnp.repeat(jnp.exp(steps), extent[position] // blocks).reshape((-1,) + (1,) * (len(extent) - position - 1))

    loudness = one(*cuts[0])
    for cut in cuts[1:]:
        loudness = loudness * one(*cut)
    return loudness


def deal_out(own_key, own, number, rows, amount, top, limit, slope):
    order = jax.random.permutation(own_key, amount)
    packed, ordinary = portions_of(amount, rows * top, limit, slope, True), portions_of(amount, rows * top, limit, slope, False)
    places = jnp.arange(amount)

    def named(lengths, offset_by):
        used = int((lengths > 0).sum())
        fixed = max(1, used // 4)
        moved = fixed + (places - fixed + offset_by * (used - fixed)) % max(1, amount - fixed)
        return jnp.zeros((amount,), jnp.int32).at[order[jnp.where(places < fixed, places, moved)]].set(jnp.asarray(lengths, jnp.int32))

    lengths = jnp.where(number % 4 == 0, named(packed, number // 4), named(ordinary, number - number // 4 - 1))
    mixed = jax.random.permutation(jax.random.fold_in(own, 3), amount)
    donor, taker = mixed[0:amount // 2 * 2:2], mixed[1:amount // 2 * 2:2]
    margin = jnp.minimum(lengths[donor] - 1, limit - lengths[taker]) // 2
    margin = jnp.where((donor == order[0]) | (taker == order[0]) | (lengths[taker] == 0), 0, jnp.maximum(margin, 0))
    moved = jax.random.randint(jax.random.fold_in(own, 4), (amount // 2,), 0, 1 << 20) % (margin + 1)
    lengths = lengths.at[donor].add(-moved).at[taker].add(moved)
    members = jnp.searchsorted(jnp.cumsum(lengths), jnp.arange(rows * top), side="right").astype(jnp.int32)
    listing = members.reshape(top, rows).T
    listing = listing[jax.random.permutation(jax.random.fold_in(own, 1), rows)]
    offset_by = jax.random.randint(jax.random.fold_in(own, 2), (rows, 1), 0, top)
    return jnp.take_along_axis(listing, (jnp.arange(top)[None, :] + offset_by) % top, axis=1)


def portions_of(count, total, reach, lean, full):
    portions = [(1 << 20) // math.isqrt(grade ** lean) + 1 for grade in range(1, count + 1)]
    largest = reach if full else min(reach, max(-(-total // count), total * portions[0] // sum(portions)))
    least = 1 if total - largest >= count - 1 else 0
    holding, spare = [largest] + [least] * (count - 1), total - largest - least * (count - 1)
    while spare > 0:
        candidates = [i for i in range(1, count) if holding[i] < largest] or [i for i in range(1, count) if holding[i] < reach]
        mass, budget = sum([portions[i] for i in candidates]), spare
        for i in candidates:
            addition = min(reach - holding[i], max(1, budget * portions[i] // mass), spare)
            holding[i] = holding[i] + addition
            spare = spare - addition
    return np.array(holding)


def centred(stream_key, shape, deviation, most, split=(), held_as=jnp.bfloat16):
    entries = jax.random.normal(stream_key, shape, jnp.float32) * deviation
    if len(split) > 0:
        entries = shard_levels(stream_key, shape, split, -0.22, 0.18) * entries
    return jnp.clip(entries, min=-most, max=most).astype(held_as)


def setup_inputs(seed: int = 0) -> dict:
    seeds = jax.random.split(jax.random.key(seed), 8)
    tokens = centred(seeds[0], (TOKENS, D), 1.0, 6.0, ((0, 64), (1, 2)))
    cotangent = centred(seeds[1], (TOKENS, D), 1.0, 6.0, ((0, 64), (1, 2)))
    experts_keys = jax.random.split(jax.random.fold_in(seeds[2], 1), TOKENS // TOK_EP)
    experts_turns = jax.random.permutation(jax.random.fold_in(seeds[2], 3), TOKENS // TOK_EP)
    experts = jax.vmap(lambda own, number: deal_out(jax.random.fold_in(seeds[2], 2), own, number, TOK_EP, EXPERTS, TOP, CAP, 2))(experts_keys, experts_turns).reshape((TOKENS, TOP))
    gate = jnp.clip(0.2 + 0.8 * jax.random.uniform(seeds[3], (TOKENS, TOP), jnp.float32) ** shard_levels(seeds[3], (TOKENS, TOP), ((0, 64),), -0.2, 0.2), 0.2, 1.0)
    w_gate = centred(seeds[4], (EXPERTS, D, F), D ** -0.5, 0.109375, ((0, 64), (2, 2)))
    w_up = centred(seeds[5], (EXPERTS, D, F), D ** -0.5, 0.109375, ((0, 64), (2, 2)))
    w_down = centred(seeds[6], (EXPERTS, F, D), F ** -0.5, 0.21875, ((0, 64), (1, 2)))
    return dict(tokens=tokens, cotangent=cotangent, experts=experts, gate=gate, w_gate=w_gate, w_up=w_up, w_down=w_down)


def slot_table(route_block, experts_count, cap):
    pair_ids = route_block.reshape(-1).astype(jnp.int32)
    pair_count = pair_ids.shape[0]
    onehot = (pair_ids[:, None] == jnp.arange(experts_count, dtype=jnp.int32)[None, :]).astype(jnp.int32)
    ranking = jnp.sum(jnp.cumsum(onehot, axis=0) * onehot, axis=1) - 1
    slot_of = (pair_ids * cap + ranking).astype(jnp.int32)
    slot_pairs = jnp.full((experts_count * cap,), pair_count, jnp.int32).at[slot_of].set(
        jnp.arange(pair_count, dtype=jnp.int32))
    return slot_of, slot_pairs


def expert_terms(rows_in, rows_cot, gate_mat, up_mat, down_mat):
    contract_last = (((1,), (1,)), ((), ()))
    contract_rows = (((0,), (0,)), ((), ()))
    gate_pre = jnp.dot(rows_in, gate_mat, preferred_element_type=jnp.float32)
    up_pre = jnp.dot(rows_in, up_mat, preferred_element_type=jnp.float32)
    sigma = jax.nn.sigmoid(gate_pre)
    active = gate_pre * sigma
    hidden = (active * up_pre).astype(jnp.bfloat16)
    hidden_grad = lax.dot_general(rows_cot, down_mat, contract_last, preferred_element_type=jnp.float32)
    products = jnp.sum(hidden.astype(jnp.float32) * hidden_grad, axis=1).astype(jnp.bfloat16)
    gate_grad_pre = (hidden_grad * up_pre * sigma * (1.0 + gate_pre * (1.0 - sigma))).astype(jnp.bfloat16)
    up_grad_pre = (hidden_grad * active).astype(jnp.bfloat16)
    block = F // N_TP
    total = jnp.zeros((rows_in.shape[0], D), jnp.float32)
    for index in range(N_TP):
        lower = index * block
        upper = lower + block
        piece = lax.dot_general(gate_grad_pre[:, lower:upper], gate_mat[:, lower:upper], contract_last,
                                preferred_element_type=jnp.float32)
        piece = piece + lax.dot_general(up_grad_pre[:, lower:upper], up_mat[:, lower:upper], contract_last,
                                        preferred_element_type=jnp.float32)
        rounded = lax.optimization_barrier(piece.astype(jnp.bfloat16))
        total = total + rounded.astype(jnp.float32)
    route_rows = total.astype(jnp.bfloat16)
    gate_sum = lax.dot_general(rows_in, gate_grad_pre, contract_rows, preferred_element_type=jnp.float32)
    up_sum = lax.dot_general(rows_in, up_grad_pre, contract_rows, preferred_element_type=jnp.float32)
    down_sum = lax.dot_general(hidden, rows_cot, contract_rows, preferred_element_type=jnp.float32)
    return (route_rows, products, gate_sum.astype(jnp.bfloat16), up_sum.astype(jnp.bfloat16),
            down_sum.astype(jnp.bfloat16), jnp.sum(gate_sum * gate_sum, axis=1),
            jnp.sum(up_sum * up_sum, axis=1), jnp.sum(down_sum * down_sum, axis=1))


def reference(tokens, cotangent, experts, gate, w_gate, w_up, w_down):
    pair_total = TOKENS * TOP
    pair_block = TOK_EP * TOP
    routes = experts.reshape(N_EP, TOK_EP, TOP)
    slot_of, slot_pairs = jax.vmap(lambda block_routes: slot_table(block_routes, EXPERTS, CAP))(routes)
    offsets = (jnp.arange(N_EP, dtype=jnp.int32) * pair_block)[:, None]
    global_pairs = jnp.where(slot_pairs < pair_block, slot_pairs + offsets, pair_total).astype(jnp.int32)
    by_expert = global_pairs.reshape(N_EP, EXPERTS, CAP).transpose(1, 0, 2).reshape(EXPERTS, N_EP * CAP)
    weighted = (gate[:, :, None] * cotangent.astype(jnp.float32)[:, None, :]).astype(jnp.bfloat16)
    padding = jnp.zeros((1, D), jnp.bfloat16)
    token_pad = jnp.concatenate([tokens, padding], axis=0)
    weighted_pad = jnp.concatenate([weighted.reshape(pair_total, D), padding], axis=0)

    def per_expert(operands):
        indices, gate_mat, up_mat, down_mat = operands
        rows_in = token_pad[indices // TOP]
        rows_cot = weighted_pad[indices]
        return expert_terms(rows_in, rows_cot, gate_mat, up_mat, down_mat)

    results = lax.map(per_expert, (by_expert, w_gate, w_up, w_down))
    route_rows, products = results[0], results[1]
    flat_index = by_expert.reshape(-1)
    pair_rows = jnp.zeros((pair_total + 1, D), jnp.bfloat16).at[flat_index].set(route_rows.reshape(-1, D))
    pair_products = jnp.zeros((pair_total + 1,), jnp.bfloat16).at[flat_index].set(products.reshape(-1))
    token_grad = jnp.sum(pair_rows[:pair_total].astype(jnp.float32).reshape(TOKENS, TOP, D), axis=1)
    gate_grad = pair_products[:pair_total].astype(jnp.float32).reshape(TOKENS, TOP) / gate
    return (token_grad.astype(jnp.bfloat16), gate_grad, results[2], results[3], results[4],
            results[5], results[6], results[7])
```

```python
import functools

import jax
import jax.numpy as jnp
from jax import lax
from jax.experimental import pallas as pl
from jax.experimental.pallas import tpu as pltpu
from jax.sharding import PartitionSpec as P

E = 64
TOK = 384
H = 1536
Q = 384
F1 = E * 8
BF = jnp.bfloat16
F32 = jnp.float32


def iota(shape, axis):
    return lax.broadcasted_iota(jnp.int32, shape, axis)


def dot(a, b):
    return lax.dot_general(a, b, (((1,), (0,)), ((), ())), preferred_element_type=F32)


def dot_last(a, b):
    return lax.dot_general(a, b, (((1,), (1,)), ((), ())), preferred_element_type=F32)


def dot_rows(a, b):
    return lax.dot_general(a, b, (((0,), (0,)), ((), ())), preferred_element_type=F32)


def ones_where(mask):
    return jnp.where(mask, 1.0, 0.0)


def named_by(exp):
    ids = iota((E, TOK), 0)
    return exp[0:1, :] == ids, exp[1:2, :] == ids


def slot_ranks(exp):
    first, second = named_by(exp)
    named = ones_where(first) + ones_where(second)
    earlier = ones_where(iota((TOK, TOK), 0) < iota((TOK, TOK), 1)).astype(BF)
    return named, dot(named.astype(BF), earlier)


def spread_rows(per_expert):
    spread = ones_where(iota((F1, E), 0) // 8 == iota((F1, E), 1)).astype(BF)
    return dot(spread, per_expert)


def row_slots(piece):
    i = iota((F1, TOK), 0) % 8
    return jnp.where(piece == 2, 16 + i % 2, i + 8 * piece).astype(F32)


def place_ranks(exp, ranks_ref):
    named, ranks = slot_ranks(exp)
    ranks_ref[...] = spread_rows(jnp.where(named > 0.5, ranks, -1.0).astype(BF))


def gathered(ranks_ref, src_ref, b):
    hit = ranks_ref[...] == row_slots(b // 4)
    return hit, dot(ones_where(hit).astype(BF), src_ref[:, pl.ds(pl.multiple_of((b % 4) * Q, Q), Q)])


def gathered_last(ranks_ref, src_ref):
    hit = ranks_ref[...] == row_slots(jnp.int32(2))
    block = (iota((F1, TOK), 0) % 8) // 2
    total = jnp.zeros((F1, Q), F32)
    for q in range(4):
        total = total + dot(
            ones_where(hit & (block == q)).astype(BF), src_ref[:, q * Q : (q + 1) * Q]
        )
    return hit, total


def send_tokens_kernel(exp_ref, src_ref, out_ref, ranks_ref):
    b = pl.program_id(0)

    @pl.when(b == 0)
    def _():
        place_ranks(exp_ref[...], ranks_ref)

    @pl.when(b < 8)
    def _():
        _, rows = gathered(ranks_ref, src_ref, b)
        out_ref[...] = rows.reshape(E, 8, Q).astype(BF)

    @pl.when(b == 8)
    def _():
        _, rows = gathered_last(ranks_ref, src_ref)
        out_ref[...] = rows.reshape(E, 8, Q).astype(BF)


def send_tokens(exp_t, tokens):
    return pl.pallas_call(
        send_tokens_kernel,
        grid=(9,),
        in_specs=[
            pl.BlockSpec((2, TOK), lambda b: (0, 0)),
            pl.BlockSpec((TOK, H), lambda b: (0, 0)),
        ],
        out_specs=pl.BlockSpec((E, 8, Q), lambda b: (0, 0, b)),
        out_shape=jax.ShapeDtypeStruct((E, 8, 9 * Q), BF),
        scratch_shapes=[pltpu.VMEM((F1, TOK), F32)],
        name="send_tokens",
    )(exp_t, tokens)


def send_cotangents_kernel(exp_ref, gate_ref, src_ref, one_ref, two_ref, ranks_ref, gates_ref, scale_ref):
    b = pl.program_id(0)

    @pl.when(b == 0)
    def _():
        exp = exp_ref[...]
        place_ranks(exp, ranks_ref)
        first, second = named_by(exp)
        gate = gate_ref[...]
        rest = jnp.where(first, gate[0:1, :], 0.0) + jnp.where(second, gate[1:2, :], 0.0)
        total = jnp.zeros((F1, TOK), F32)
        for _ in range(3):
            part = rest.astype(BF)
            rest = rest - part.astype(F32)
            total = total + spread_rows(part)
        gates_ref[...] = total

    @pl.when((b % 4 == 0))
    def _():
        hit = ranks_ref[...] == row_slots(b // 4)
        scale = jnp.sum(jnp.where(hit, gates_ref[...], 0.0), axis=1, keepdims=True)
        scale_ref[...] = jnp.broadcast_to(scale, (F1, 128))

    def scaled(rows):
        return (rows * scale_ref[:, 0:1]).reshape(E, 8, Q).astype(BF)

    @pl.when(b < 4)
    def _():
        one_ref[...] = scaled(gathered(ranks_ref, src_ref, b)[1])

    @pl.when((b >= 4) & (b < 8))
    def _():
        two_ref[...] = scaled(gathered(ranks_ref, src_ref, b)[1])

    @pl.when(b == 8)
    def _():
        two_ref[...] = scaled(gathered_last(ranks_ref, src_ref)[1])


def send_cotangents(exp_t, gate_t, cotangent):
    return pl.pallas_call(
        send_cotangents_kernel,
        grid=(9,),
        in_specs=[
            pl.BlockSpec((2, TOK), lambda b: (0, 0)),
            pl.BlockSpec((2, TOK), lambda b: (0, 0)),
            pl.BlockSpec((TOK, H), lambda b: (0, 0)),
        ],
        out_specs=[
            pl.BlockSpec((E, 8, Q), lambda b: (0, 0, jnp.minimum(b, 3))),
            pl.BlockSpec((E, 8, Q), lambda b: (0, 0, jnp.maximum(b - 4, 0))),
        ],
        out_shape=[
            jax.ShapeDtypeStruct((E, 8, 4 * Q), BF),
            jax.ShapeDtypeStruct((E, 8, 5 * Q), BF),
        ],
        scratch_shapes=[
            pltpu.VMEM((F1, TOK), F32),
            pltpu.VMEM((F1, TOK), F32),
            pltpu.VMEM((F1, 128), F32),
        ],
        name="send_cotangents",
    )(exp_t, gate_t, cotangent)


def unpack_last(last):
    flat = last.astype(F32).reshape(F1, Q).astype(BF)
    row = iota((128, F1), 0)
    pieces = []
    for q in range(4):
        pick = ones_where(row // 2 * 8 + 2 * q + row % 2 == iota((128, F1), 1)).astype(BF)
        pieces.append(dot(pick, flat).astype(BF))
    return pieces


def unpack_kernel(steps, core_ref, own_ref, other_ref, own_last_ref, other_last_ref, out_ref):
    b = pl.program_id(0)
    core = core_ref[0]
    sides = ((core, own_ref, own_last_ref), (1 - core, other_ref, other_last_ref))

    @pl.when(b < steps)
    def _():
        for half, rows_ref, _ in sides:
            rows = rows_ref[...].astype(F32).reshape(128, H).astype(BF)
            out_ref[:, pl.ds(pl.multiple_of(half * H, H), H)] = rows

    @pl.when(b == steps)
    def _():
        for half, _, last_ref in sides:
            for q, piece in enumerate(unpack_last(last_ref[...])):
                out_ref[:, pl.ds(pl.multiple_of(half * H + q * Q, Q), Q)] = piece


def unpack(core, own, other):
    wide = (own.shape[2] - Q) // H
    steps = 4 * wide

    def rows_at(b):
        bb = jnp.minimum(b, steps - 1)
        return (bb % 4, 0, bb // 4)

    rows = pl.BlockSpec((16, 8, H), rows_at)
    last = pl.BlockSpec((E, 8, Q), lambda b: (0, 0, wide * 4))
    return pl.pallas_call(
        functools.partial(unpack_kernel, steps),
        grid=(steps + 1,),
        in_specs=[pl.BlockSpec(memory_space=pltpu.SMEM), rows, rows, last, last],
        out_specs=pl.BlockSpec((128, 2 * H), lambda b: (b, 0)),
        out_shape=jax.ShapeDtypeStruct((steps * 128 + 128, 2 * H), BF),
        name="unpack",
    )(core, own, other, own, other)


def pack_kernel(mine_ref, got_ref, mine_last_ref, got_last_ref, prod_ref, out_ref):
    b = pl.program_id(0)

    @pl.when(b < 4)
    def _():
        total = mine_ref[...].astype(F32) + got_ref[...].astype(F32)
        out_ref[...] = total.reshape(E, 8, Q).astype(BF)

    @pl.when(b == 4)
    def _():
        total = (mine_last_ref[...].astype(F32) + got_last_ref[...].astype(F32)).astype(BF)
        col = iota((F1, 128), 1)
        row = iota((F1, 128), 0)
        packed = jnp.zeros((F1, Q), F32)
        for q in range(4):
            pick = ones_where(col // 2 * 8 + 2 * q + col % 2 == row).astype(BF)
            packed = packed + dot(pick, total[:, q * Q : (q + 1) * Q])
        out_ref[...] = packed.reshape(E, 8, Q).astype(BF)

    @pl.when(b == 5)
    def _():
        out_ref[...] = jnp.zeros((E, 8, Q), BF)
        out_ref[:, :, 0:128] = prod_ref[...]


def pack(mine, got, prods):
    main = pl.BlockSpec((F1, Q), lambda b: (0, jnp.minimum(b, 3)))
    last = pl.BlockSpec((128, H), lambda b: (4, 0))
    return pl.pallas_call(
        pack_kernel,
        grid=(6,),
        in_specs=[main, main, last, last, pl.BlockSpec((E, 8, 128), lambda b: (0, 0, 0))],
        out_specs=pl.BlockSpec((E, 8, Q), lambda b: (0, 0, b)),
        out_shape=jax.ShapeDtypeStruct((E, 8, 5 * Q + 128), BF),
        name="pack",
    )(mine, got, mine, got, prods)


def combine_kernel(exp_ref, gate_ref, one_ref, two_ref, last_ref, prod_ref, out_ref, gate_out_ref, ranks_ref):
    b = pl.program_id(0)
    exp = exp_ref[...]

    @pl.when(b == 0)
    def _():
        place_ranks(exp, ranks_ref)
        named, ranks = slot_ranks(exp)
        flat = prod_ref[...].astype(F32).reshape(F1, 128).astype(BF)
        i = iota((F1, TOK), 0) % 8
        for k, mask in enumerate(named_by(exp)):
            mine = spread_rows(jnp.where(mask, ranks, -1.0).astype(BF))
            total = jnp.zeros((1, TOK), F32)
            for piece in range(3):
                hit = mine == row_slots(jnp.int32(piece))
                if piece == 2:
                    hit = hit & (i < 2)
                found = lax.dot_general(
                    flat, ones_where(hit).astype(BF), (((0,), (0,)), ((), ())), preferred_element_type=F32
                )
                total = total + found[piece : piece + 1, :]
            gate_out_ref[k : k + 1, :] = total / gate_ref[k : k + 1, :]

    def hits(piece):
        return ones_where(ranks_ref[...] == row_slots(jnp.int32(piece))).astype(BF)

    def flat(ref):
        return ref[...].astype(F32).reshape(F1, Q).astype(BF)

    block = (iota((F1, TOK), 0) % 8) // 2
    last = ranks_ref[...] == row_slots(jnp.int32(2))
    total = dot_rows(hits(0), flat(one_ref)) + dot_rows(hits(1), flat(two_ref))
    total = total + dot_rows(ones_where(last & (block == b)).astype(BF), flat(last_ref))
    out_ref[...] = total.astype(BF)


def combine(exp_t, gate_t, one, two):
    small = pl.BlockSpec((2, TOK), lambda b: (0, 0))
    return pl.pallas_call(
        combine_kernel,
        grid=(4,),
        in_specs=[
            small,
            small,
            pl.BlockSpec((E, 8, Q), lambda b: (0, 0, b)),
            pl.BlockSpec((E, 8, Q), lambda b: (0, 0, b)),
            pl.BlockSpec((E, 8, Q), lambda b: (0, 0, 4)),
            pl.BlockSpec((E, 8, 128), lambda b: (0, 0, 15)),
        ],
        out_specs=[pl.BlockSpec((TOK, Q), lambda b: (0, b)), small],
        out_shape=[jax.ShapeDtypeStruct((TOK, H), BF), jax.ShapeDtypeStruct((2, TOK), F32)],
        scratch_shapes=[pltpu.VMEM((F1, TOK), F32)],
        name="combine",
    )(exp_t, gate_t, one, two, two, two)


def to_experts(x):
    return lax.all_to_all(x, "ep", split_axis=0, concat_axis=0, tiled=True)


def swap_cores(x):
    return lax.ppermute(x, "tp", [(0, 1), (1, 0)])


def per_device(tokens, cotangent, experts, gate, w_gate, w_up, w_down):
    core = lax.axis_index("tp").astype(jnp.int32)
    core_arg = core.reshape(1)
    exp_t, gate_t = experts.T, gate.T
    gate_mat, up_mat, down_mat = w_gate[0], w_up[0], w_down[0]

    tok_own = to_experts(send_tokens(exp_t, tokens))
    cot_one, cot_two = send_cotangents(exp_t, gate_t, cotangent)
    cot_one, cot_two = to_experts(cot_one), to_experts(cot_two)

    rows_in = unpack(core_arg, tok_own, swap_cores(tok_own))
    gate_pre = dot(rows_in, gate_mat)
    up_pre = dot(rows_in, up_mat)
    sigma = jax.nn.sigmoid(gate_pre)
    active = gate_pre * sigma
    hidden = (active * up_pre).astype(BF)
    gate_slope = up_pre * sigma * (1.0 + gate_pre * (1.0 - sigma))

    def half(mat, index, axis):
        return lax.dynamic_slice_in_dim(mat, index * H, H, axis)

    def chunk(rows, lo, hi):
        grad = rows[0]
        for part in rows[1:]:
            grad = grad + part
        parts = jnp.sum(hidden[lo:hi].astype(F32) * grad, axis=1)
        gate_grad_pre = (grad * gate_slope[lo:hi]).astype(BF)
        up_grad_pre = (grad * active[lo:hi]).astype(BF)

        def partial(index):
            return (
                dot_last(gate_grad_pre, half(gate_mat, index, 0))
                + dot_last(up_grad_pre, half(up_mat, index, 0))
            ).astype(BF)

        sent = swap_cores(partial(1 - core))
        return parts, gate_grad_pre, up_grad_pre, partial(core), sent

    own = cot_one.reshape(F1, H)
    other = swap_cores(cot_one).reshape(F1, H)
    down_own, down_other = half(down_mat, core, 1), half(down_mat, 1 - core, 1)
    one = chunk((dot_last(own, down_own), dot_last(other, down_other)), 0, F1)
    back_one = (one[3].astype(F32) + one[4].astype(F32)).astype(BF)
    back_one = to_experts(back_one.reshape(E, 8, H))

    rows_two = unpack(core_arg, cot_two, swap_cores(cot_two))
    two = chunk((dot_last(rows_two, down_mat),), F1, 1152)
    parts = jnp.concatenate([one[0], two[0]])
    products = (parts + swap_cores(parts)).astype(BF)
    first, second, third = products[:F1], products[F1 : 2 * F1], products[2 * F1 :]
    third = jnp.pad(third.reshape(E, 2), ((0, 0), (0, 6)))
    prods = jnp.stack([first.reshape(E, 8), second.reshape(E, 8), third], axis=2)
    prods = jnp.pad(prods, ((0, 0), (0, 0), (0, 125)))
    back_two = to_experts(pack(two[3], two[4], prods))

    gate_grad_pre = jnp.concatenate([one[1], two[1]])
    up_grad_pre = jnp.concatenate([one[2], two[2]])
    gate_sum = dot_rows(rows_in, gate_grad_pre)
    up_sum = dot_rows(rows_in, up_grad_pre)
    norms = jnp.stack([jnp.sum(gate_sum * gate_sum, axis=1), jnp.sum(up_sum * up_sum, axis=1)])
    norms = norms + swap_cores(norms)
    down_own = dot_rows(hidden[:F1], own)
    down_other = dot_rows(hidden[:F1], other)
    down_one = jnp.where(
        core == 0,
        jnp.concatenate([down_own, down_other], axis=1),
        jnp.concatenate([down_other, down_own], axis=1),
    )
    down_sum = down_one + dot_rows(hidden[F1:], rows_two)
    down_norms = jnp.sum(down_sum * down_sum, axis=1)

    token_grad, gate_grad_t = combine(exp_t, gate_t, back_one, back_two)
    return (
        token_grad,
        gate_grad_t.T,
        gate_sum.astype(BF)[None],
        up_sum.astype(BF)[None],
        down_sum.astype(BF)[None],
        norms[0:1],
        norms[1:2],
        down_norms[None],
    )


def solution(mesh):
    placed = (
        P("ep", "tp"),
        P("ep", "tp"),
        P("ep", None),
        P("ep", None),
        P("ep", None, "tp"),
        P("ep", None, "tp"),
        P("ep", "tp", None),
    )
    return jax.shard_map(
        per_device,
        mesh=mesh,
        in_specs=placed,
        out_specs=(
            P("ep", "tp"),
            P("ep", None),
            P("ep", None, "tp"),
            P("ep", None, "tp"),
            P("ep", "tp", None),
            P("ep", None),
            P("ep", None),
            P("ep", "tp"),
        ),
        check_vma=False,
    )
```

```python
import functools

import jax
import jax.numpy as jnp
from jax import lax
from jax.experimental import pallas as pl
from jax.experimental.pallas import tpu as pltpu
from jax.sharding import PartitionSpec as P


E = 64
TOK = 384
H = 1536
Q = 384
F1 = E * 8
BF = jnp.bfloat16
F32 = jnp.float32


def iota(shape, axis):
    return lax.broadcasted_iota(jnp.int32, shape, axis)


def dot(a, b):
    return lax.dot_general(a, b, (((1,), (0,)), ((), ())), preferred_element_type=F32)


def dot_last(a, b):
    return lax.dot_general(a, b, (((1,), (1,)), ((), ())), preferred_element_type=F32)


def dot_rows(a, b):
    return lax.dot_general(a, b, (((0,), (0,)), ((), ())), preferred_element_type=F32)


def ones_where(mask):
    return jnp.where(mask, 1.0, 0.0)


def named_by(exp):
    ids = iota((E, TOK), 0)
    return exp[0:1, :] == ids, exp[1:2, :] == ids


def slot_ranks(exp):
    first, second = named_by(exp)
    named = ones_where(first) + ones_where(second)
    earlier = ones_where(iota((TOK, TOK), 0) < iota((TOK, TOK), 1)).astype(BF)
    return named, dot(named.astype(BF), earlier)


def spread_rows(per_expert):
    spread = ones_where(iota((F1, E), 0) // 8 == iota((F1, E), 1)).astype(BF)
    return dot(spread, per_expert)


def row_slots(piece):
    i = iota((F1, TOK), 0) % 8
    return jnp.where(piece == 2, 16 + i % 2, i + 8 * piece).astype(F32)


def routes_kernel(exp_ref, gate_ref, ranks_ref, gates_ref):
    exp = exp_ref[...]
    named, ranks = slot_ranks(exp)
    ranks_ref[...] = spread_rows(jnp.where(named > 0.5, ranks, -1.0).astype(BF))
    first, second = named_by(exp)
    gate = gate_ref[...]
    rest = jnp.where(first, gate[0:1, :], 0.0) + jnp.where(second, gate[1:2, :], 0.0)
    total = jnp.zeros((F1, TOK), F32)
    for _ in range(3):
        part = rest.astype(BF)
        rest = rest - part.astype(F32)
        total = total + spread_rows(part)
    gates_ref[...] = total


def routes(exp_t, gate_t):
    shape = jax.ShapeDtypeStruct((F1, TOK), F32)
    return pl.pallas_call(routes_kernel, out_shape=[shape, shape], name="routes")(exp_t, gate_t)


def send_kernel(lo, last, scaled, *refs):
    ranks_ref, gates_ref, src_ref, out_ref = refs[:4] if scaled else (refs[0], None, *refs[1:3])
    b = pl.program_id(0) + lo

    def scale(hit, rows):
        if scaled:
            rows = rows * jnp.sum(jnp.where(hit, gates_ref[...], 0.0), axis=1, keepdims=True)
        return rows.reshape(E, 8, Q).astype(BF)

    @pl.when(b < 8)
    def _():
        hit = ranks_ref[...] == row_slots(b // 4)
        src = src_ref[:, pl.ds(pl.multiple_of((b % 4) * Q, Q), Q)]
        out_ref[...] = scale(hit, dot(ones_where(hit).astype(BF), src))

    if last:

        @pl.when(b == 8)
        def _():
            hit = ranks_ref[...] == row_slots(jnp.int32(2))
            block = (iota((F1, TOK), 0) % 8) // 2
            total = jnp.zeros((F1, Q), F32)
            for q in range(4):
                pick = ones_where(hit & (block == q)).astype(BF)
                total = total + dot(pick, src_ref[:, q * Q : (q + 1) * Q])
            out_ref[...] = scale(hit, total)


def send(tables, src, lo, hi):
    whole = pl.BlockSpec((F1, TOK), lambda b: (0, 0))
    return pl.pallas_call(
        functools.partial(send_kernel, lo, hi == 9, len(tables) == 2),
        grid=(hi - lo,),
        in_specs=[whole] * len(tables) + [pl.BlockSpec((TOK, H), lambda b: (0, 0))],
        out_specs=pl.BlockSpec((E, 8, Q), lambda b: (0, 0, b)),
        out_shape=jax.ShapeDtypeStruct((E, 8, (hi - lo) * Q), BF),
        name="send",
    )(*tables, src)


def unpack_last(last):
    flat = last.astype(F32).reshape(F1, Q).astype(BF)
    row = iota((128, F1), 0)
    pieces = []
    for q in range(4):
        pick = ones_where(row // 2 * 8 + 2 * q + row % 2 == iota((128, F1), 1)).astype(BF)
        pieces.append(dot(pick, flat).astype(BF))
    return pieces


def unpack_kernel(steps, core_ref, own_ref, other_ref, own_last_ref, other_last_ref, out_ref):
    b = pl.program_id(0)
    core = core_ref[0]
    sides = ((core, own_ref, own_last_ref), (1 - core, other_ref, other_last_ref))

    @pl.when(b < steps)
    def _():
        for half, rows_ref, _ in sides:
            rows = rows_ref[...].astype(F32).reshape(128, H).astype(BF)
            out_ref[:, pl.ds(pl.multiple_of(half * H, H), H)] = rows

    @pl.when(b == steps)
    def _():
        for half, _, last_ref in sides:
            for q, piece in enumerate(unpack_last(last_ref[...])):
                out_ref[:, pl.ds(pl.multiple_of(half * H + q * Q, Q), Q)] = piece


def unpack(core, own, other):
    wide = (own.shape[2] - Q) // H
    steps = 4 * wide

    def rows_at(b):
        bb = jnp.minimum(b, steps - 1)
        return (bb % 4, 0, bb // 4)

    rows = pl.BlockSpec((16, 8, H), rows_at)
    last = pl.BlockSpec((E, 8, Q), lambda b: (0, 0, wide * 4))
    return pl.pallas_call(
        functools.partial(unpack_kernel, steps),
        grid=(steps + 1,),
        in_specs=[pl.BlockSpec(memory_space=pltpu.SMEM), rows, rows, last, last],
        out_specs=pl.BlockSpec((128, 2 * H), lambda b: (b, 0)),
        out_shape=jax.ShapeDtypeStruct((steps * 128 + 128, 2 * H), BF),
        name="unpack",
    )(core, own, other, own, other)


def pack_kernel(mine_ref, got_ref, mine_last_ref, got_last_ref, prod_ref, out_ref):
    b = pl.program_id(0)

    @pl.when(b < 4)
    def _():
        total = mine_ref[...].astype(F32) + got_ref[...].astype(F32)
        out_ref[...] = total.reshape(E, 8, Q).astype(BF)

    @pl.when(b == 4)
    def _():
        total = (mine_last_ref[...].astype(F32) + got_last_ref[...].astype(F32)).astype(BF)
        col = iota((F1, 128), 1)
        row = iota((F1, 128), 0)
        packed = jnp.zeros((F1, Q), F32)
        for q in range(4):
            pick = ones_where(col // 2 * 8 + 2 * q + col % 2 == row).astype(BF)
            packed = packed + dot(pick, total[:, q * Q : (q + 1) * Q])
        out_ref[...] = packed.reshape(E, 8, Q).astype(BF)

    @pl.when(b == 5)
    def _():
        out_ref[...] = jnp.zeros((E, 8, Q), BF)
        out_ref[:, :, 0:128] = prod_ref[...]


def pack(mine, got, prods):
    main = pl.BlockSpec((F1, Q), lambda b: (0, jnp.minimum(b, 3)))
    last = pl.BlockSpec((128, H), lambda b: (4, 0))
    return pl.pallas_call(
        pack_kernel,
        grid=(6,),
        in_specs=[main, main, last, last, pl.BlockSpec((E, 8, 128), lambda b: (0, 0, 0))],
        out_specs=pl.BlockSpec((E, 8, Q), lambda b: (0, 0, b)),
        out_shape=jax.ShapeDtypeStruct((E, 8, 5 * Q + 128), BF),
        name="pack",
    )(mine, got, mine, got, prods)


def combine_kernel(ranks_ref, exp_ref, gate_ref, one_ref, two_ref, last_ref, prod_ref, out_ref, gate_out_ref):
    b = pl.program_id(0)

    @pl.when(b == 0)
    def _():
        exp = exp_ref[...]
        _, ranks = slot_ranks(exp)
        flat = prod_ref[...].astype(F32).reshape(F1, 128).astype(BF)
        i = iota((F1, TOK), 0) % 8
        for k, mask in enumerate(named_by(exp)):
            mine = spread_rows(jnp.where(mask, ranks, -1.0).astype(BF))
            total = jnp.zeros((1, TOK), F32)
            for piece in range(3):
                hit = mine == row_slots(jnp.int32(piece))
                if piece == 2:
                    hit = hit & (i < 2)
                found = lax.dot_general(
                    flat, ones_where(hit).astype(BF), (((0,), (0,)), ((), ())), preferred_element_type=F32
                )
                total = total + found[piece : piece + 1, :]
            gate_out_ref[k : k + 1, :] = total / gate_ref[k : k + 1, :]

    def hits(piece):
        return ones_where(ranks_ref[...] == row_slots(jnp.int32(piece))).astype(BF)

    def flat(ref):
        return ref[...].astype(F32).reshape(F1, Q).astype(BF)

    block = (iota((F1, TOK), 0) % 8) // 2
    last = ranks_ref[...] == row_slots(jnp.int32(2))
    total = dot_rows(hits(0), flat(one_ref)) + dot_rows(hits(1), flat(two_ref))
    total = total + dot_rows(ones_where(last & (block == b)).astype(BF), flat(last_ref))
    out_ref[...] = total.astype(BF)


def combine(ranks, exp_t, gate_t, one, two):
    small = pl.BlockSpec((2, TOK), lambda b: (0, 0))
    return pl.pallas_call(
        combine_kernel,
        grid=(4,),
        in_specs=[
            pl.BlockSpec((F1, TOK), lambda b: (0, 0)),
            small,
            small,
            pl.BlockSpec((E, 8, Q), lambda b: (0, 0, b)),
            pl.BlockSpec((E, 8, Q), lambda b: (0, 0, b)),
            pl.BlockSpec((E, 8, Q), lambda b: (0, 0, 4)),
            pl.BlockSpec((E, 8, 128), lambda b: (0, 0, 15)),
        ],
        out_specs=[pl.BlockSpec((TOK, Q), lambda b: (0, b)), small],
        out_shape=[jax.ShapeDtypeStruct((TOK, H), BF), jax.ShapeDtypeStruct((2, TOK), F32)],
        name="combine",
    )(ranks, exp_t, gate_t, one, two, two, two)


def to_experts(x):
    return lax.all_to_all(x, "ep", split_axis=0, concat_axis=0, tiled=True)


def swap_cores(x):
    return lax.ppermute(x, "tp", [(0, 1), (1, 0)])


def half(mat, index, axis):
    return lax.dynamic_slice_in_dim(mat, index * H, H, axis)


def step(tokens, cotangent, experts, gate, w_gate, w_up, w_down):
    core = lax.axis_index("tp").astype(jnp.int32)
    core_arg = core.reshape(1)
    gate_mat, up_mat, down_mat = w_gate[0], w_up[0], w_down[0]
    exp_t, gate_t = experts.T, gate.T
    gates = [half(gate_mat, index, 0) for index in (core, 1 - core)]
    ups = [half(up_mat, index, 0) for index in (core, 1 - core)]
    downs = [half(down_mat, index, 1) for index in (core, 1 - core)]
    ranks, gates_of = routes(exp_t, gate_t)
    tok_own = send((ranks,), tokens, 0, 9)
    tok_own = to_experts(tok_own)
    cot_one = send((ranks, gates_of), cotangent, 0, 4)
    cot_one = to_experts(cot_one)
    cot_two = send((ranks, gates_of), cotangent, 4, 9)
    cot_two = to_experts(cot_two)
    tok_other = swap_cores(tok_own)

    rows_in = unpack(core_arg, tok_own, tok_other)
    gate_pre = dot(rows_in, gate_mat)
    up_pre = dot(rows_in, up_mat)
    sigma = jax.nn.sigmoid(gate_pre)
    active = gate_pre * sigma
    hidden = (active * up_pre).astype(BF)
    gate_slope = up_pre * sigma * (1.0 + gate_pre * (1.0 - sigma))

    def chunk(rows, lo, hi):
        grad = rows[0]
        for part in rows[1:]:
            grad = grad + part
        parts = jnp.sum(hidden[lo:hi].astype(F32) * grad, axis=1)
        gate_grad_pre = (grad * gate_slope[lo:hi]).astype(BF)
        up_grad_pre = (grad * active[lo:hi]).astype(BF)

        def partial(index):
            return (dot_last(gate_grad_pre, gates[index]) + dot_last(up_grad_pre, ups[index])).astype(BF)

        sent = swap_cores(partial(1))
        return parts, gate_grad_pre, up_grad_pre, partial(0), sent

    cot_one_other = swap_cores(cot_one)
    own = cot_one.reshape(F1, H)
    other = cot_one_other.reshape(F1, H)
    one = chunk((dot_last(own, downs[0]), dot_last(other, downs[1])), 0, F1)
    back_one = (one[3].astype(F32) + one[4].astype(F32)).astype(BF).reshape(E, 8, H)
    back_one = to_experts(back_one)

    cot_two_other = swap_cores(cot_two)
    rows_two = unpack(core_arg, cot_two, cot_two_other)
    two = chunk((dot_last(rows_two, down_mat),), F1, 1152)
    parts = jnp.concatenate([one[0], two[0]])
    products = (parts + swap_cores(parts)).astype(BF)
    first, second, third = products[:F1], products[F1 : 2 * F1], products[2 * F1 :]
    third = jnp.pad(third.reshape(E, 2), ((0, 0), (0, 6)))
    prods = jnp.stack([first.reshape(E, 8), second.reshape(E, 8), third], axis=2)
    prods = jnp.pad(prods, ((0, 0), (0, 0), (0, 125)))
    back_two = pack(two[3], two[4], prods)
    back_two = to_experts(back_two)

    gate_grad_pre = jnp.concatenate([one[1], two[1]])
    up_grad_pre = jnp.concatenate([one[2], two[2]])
    gate_sum = dot_rows(rows_in, gate_grad_pre)
    up_sum = dot_rows(rows_in, up_grad_pre)
    norms = jnp.stack([jnp.sum(gate_sum * gate_sum, axis=1), jnp.sum(up_sum * up_sum, axis=1)])
    norms = norms + swap_cores(norms)
    down_own = dot_rows(hidden[:F1], own)
    down_other = dot_rows(hidden[:F1], other)
    down_one = jnp.where(
        core == 0,
        jnp.concatenate([down_own, down_other], axis=1),
        jnp.concatenate([down_other, down_own], axis=1),
    )
    down_sum = down_one + dot_rows(hidden[F1:], rows_two)
    down_norms = jnp.sum(down_sum * down_sum, axis=1)

    token_grad, gate_grad_t = combine(ranks, exp_t, gate_t, back_one, back_two)
    return (
        token_grad,
        gate_grad_t.T,
        gate_sum.astype(BF)[None],
        up_sum.astype(BF)[None],
        down_sum.astype(BF)[None],
        norms[0:1],
        norms[1:2],
        down_norms[None],
    )


def solution(mesh):
    placed = (
        P("ep", "tp"),
        P("ep", "tp"),
        P("ep", None),
        P("ep", None),
        P("ep", None, "tp"),
        P("ep", None, "tp"),
        P("ep", "tp", None),
    )
    return jax.shard_map(
        step,
        mesh=mesh,
        in_specs=placed,
        out_specs=(
            P("ep", "tp"),
            P("ep", None),
            P("ep", None, "tp"),
            P("ep", None, "tp"),
            P("ep", "tp", None),
            P("ep", None),
            P("ep", None),
            P("ep", "tp"),
        ),
        check_vma=False,
    )
```

```python
import functools

import jax
import jax.numpy as jnp
from jax import lax
from jax.experimental import pallas as pl
from jax.experimental.pallas import tpu as pltpu
from jax.sharding import PartitionSpec as P


E = 64
TOK = 384
H = 1536
Q = 384
F1 = E * 8
BF = jnp.bfloat16
F32 = jnp.float32


def iota(shape, axis):
    return lax.broadcasted_iota(jnp.int32, shape, axis)


def dot(a, b):
    return lax.dot_general(a, b, (((1,), (0,)), ((), ())), preferred_element_type=F32)


def dot_last(a, b):
    return lax.dot_general(a, b, (((1,), (1,)), ((), ())), preferred_element_type=F32)


def dot_rows(a, b):
    return lax.dot_general(a, b, (((0,), (0,)), ((), ())), preferred_element_type=F32)


def ones_where(mask):
    return jnp.where(mask, 1.0, 0.0)


def named_by(exp):
    ids = iota((E, TOK), 0)
    return exp[0:1, :] == ids, exp[1:2, :] == ids


def slot_ranks(exp):
    first, second = named_by(exp)
    named = ones_where(first) + ones_where(second)
    earlier = ones_where(iota((TOK, TOK), 0) < iota((TOK, TOK), 1)).astype(BF)
    return named, dot(named.astype(BF), earlier)


def spread_rows(per_expert):
    spread = ones_where(iota((F1, E), 0) // 8 == iota((F1, E), 1)).astype(BF)
    return dot(spread, per_expert)


def row_slots(piece):
    i = iota((F1, TOK), 0) % 8
    return jnp.where(piece == 2, 16 + i % 2, i + 8 * piece).astype(F32)


def put_last(rows):
    row = iota((F1, 128), 0)
    col = iota((F1, 128), 1)
    total = jnp.zeros((F1, Q), F32)
    for q in range(4):
        place = ones_where(row == col // 2 * 8 + 2 * q + col % 2).astype(BF)
        total = total + dot(place, rows[:, q * Q : (q + 1) * Q])
    return total


def send_tokens_kernel(exp_ref, gate_ref, src_ref, out_ref, ranks_ref, gates_ref, small_ref):
    b = pl.program_id(0)

    @pl.when(b == 0)
    def _():
        exp = exp_ref[...]
        named, ranks = slot_ranks(exp)
        small = jnp.where(named > 0.5, ranks, -1.0).astype(BF)
        small_ref[...] = small
        ranks_ref[...] = spread_rows(small)

    def rows(piece, lo, hi):
        hit = ones_where(ranks_ref[...] == row_slots(jnp.int32(piece))).astype(BF)
        return dot(hit, src_ref[:, lo:hi]).reshape(E, 8, hi - lo).astype(BF)

    @pl.when(b == 0)
    def _():
        out_ref[...] = rows(0, 0, 1152)

    @pl.when(b == 1)
    def _():
        out_ref[:, :, 0:384] = rows(0, 1152, 1536)
        out_ref[:, :, 384:1152] = rows(1, 0, 768)

    @pl.when(b == 2)
    def _():
        out_ref[:, :, 0:768] = rows(1, 768, 1536)
        row = iota((128, E), 0)
        spread = ones_where(row // 2 == iota((128, E), 1)).astype(BF)
        slot = (16 + iota((128, TOK), 0) % 2).astype(F32)
        hit = ones_where(dot(spread, small_ref[...]) == slot).astype(BF)
        last = dot(hit, src_ref[...]).astype(BF)
        out_ref[:, :, 768:1152] = put_last(last).reshape(E, 8, Q).astype(BF)
        first, second = named_by(exp_ref[...])
        gate = gate_ref[...]
        rest = jnp.where(first, gate[0:1, :], 0.0) + jnp.where(second, gate[1:2, :], 0.0)
        total = jnp.zeros((F1, TOK), F32)
        for _ in range(3):
            part = rest.astype(BF)
            rest = rest - part.astype(F32)
            total = total + spread_rows(part)
        gates_ref[...] = total


def send_tokens(exp_t, gate_t, tokens):
    small = pl.BlockSpec((2, TOK), lambda b: (0, 0))
    table = pl.BlockSpec((F1, TOK), lambda b: (0, 0))
    shape = jax.ShapeDtypeStruct((F1, TOK), F32)
    return pl.pallas_call(
        send_tokens_kernel,
        grid=(3,),
        in_specs=[small, small, pl.BlockSpec((TOK, H), lambda b: (0, 0))],
        out_specs=[pl.BlockSpec((E, 8, 1152), lambda b: (0, 0, b)), table, table],
        out_shape=[jax.ShapeDtypeStruct((E, 8, 3456), BF), shape, shape],
        scratch_shapes=[pltpu.VMEM((E, TOK), BF)],
        name="send_tokens",
    )(exp_t, gate_t, tokens)


def send_kernel(lo, last, ranks_ref, gates_ref, src_ref, out_ref):
    b = pl.program_id(0) + lo

    def scaled(hit, rows):
        rows = rows * jnp.sum(jnp.where(hit, gates_ref[...], 0.0), axis=1, keepdims=True)
        return rows.reshape(E, 8, Q).astype(BF)

    @pl.when(b < 8)
    def _():
        hit = ranks_ref[...] == row_slots(b // 4)
        src = src_ref[:, pl.ds(pl.multiple_of((b % 4) * Q, Q), Q)]
        out_ref[...] = scaled(hit, dot(ones_where(hit).astype(BF), src))

    if last:

        @pl.when(b == 8)
        def _():
            hit = ranks_ref[...] == row_slots(jnp.int32(2))
            block = (iota((F1, TOK), 0) % 8) // 2
            total = jnp.zeros((F1, Q), F32)
            for q in range(4):
                pick = ones_where(hit & (block == q)).astype(BF)
                total = total + dot(pick, src_ref[:, q * Q : (q + 1) * Q])
            out_ref[...] = scaled(hit, total)


def send(ranks, gates, src, lo, hi):
    whole = pl.BlockSpec((F1, TOK), lambda b: (0, 0))
    return pl.pallas_call(
        functools.partial(send_kernel, lo, hi == 9),
        grid=(hi - lo,),
        in_specs=[whole, whole, pl.BlockSpec((TOK, H), lambda b: (0, 0))],
        out_specs=pl.BlockSpec((E, 8, Q), lambda b: (0, 0, b)),
        out_shape=jax.ShapeDtypeStruct((E, 8, (hi - lo) * Q), BF),
        name="send",
    )(ranks, gates, src)


def unpack_last(last):
    flat = last.astype(F32).reshape(F1, Q).astype(BF)
    row = iota((128, F1), 0)
    pieces = []
    for q in range(4):
        pick = ones_where(row // 2 * 8 + 2 * q + row % 2 == iota((128, F1), 1)).astype(BF)
        pieces.append(dot(pick, flat).astype(BF))
    return pieces


def unpack_kernel(steps, core_ref, own_ref, other_ref, own_last_ref, other_last_ref, out_ref):
    b = pl.program_id(0)
    core = core_ref[0]
    sides = ((core, own_ref, own_last_ref), (1 - core, other_ref, other_last_ref))

    @pl.when(b < steps)
    def _():
        for half, rows_ref, _ in sides:
            rows = rows_ref[...].astype(F32).reshape(128, H).astype(BF)
            out_ref[:, pl.ds(pl.multiple_of(half * H, H), H)] = rows

    @pl.when(b == steps)
    def _():
        for half, _, last_ref in sides:
            for q, piece in enumerate(unpack_last(last_ref[...])):
                out_ref[:, pl.ds(pl.multiple_of(half * H + q * Q, Q), Q)] = piece


def unpack(core, own, other):
    wide = (own.shape[2] - Q) // H
    steps = 4 * wide

    def rows_at(b):
        bb = jnp.minimum(b, steps - 1)
        return (bb % 4, 0, bb // 4)

    rows = pl.BlockSpec((16, 8, H), rows_at)
    last = pl.BlockSpec((E, 8, Q), lambda b: (0, 0, wide * 4))
    return pl.pallas_call(
        functools.partial(unpack_kernel, steps),
        grid=(steps + 1,),
        in_specs=[pl.BlockSpec(memory_space=pltpu.SMEM), rows, rows, last, last],
        out_specs=pl.BlockSpec((128, 2 * H), lambda b: (b, 0)),
        out_shape=jax.ShapeDtypeStruct((steps * 128 + 128, 2 * H), BF),
        name="unpack",
    )(core, own, other, own, other)


def pack_kernel(mine_ref, got_ref, mine_last_ref, got_last_ref, part_ref, got_part_ref, out_ref):
    b = pl.program_id(0)

    @pl.when(b < 3)
    def _():
        total = mine_ref[...].astype(F32) + got_ref[...].astype(F32)
        out_ref[...] = total.reshape(E, 8, 512).astype(BF)

    @pl.when(b == 3)
    def _():
        total = (mine_last_ref[...].astype(F32) + got_last_ref[...].astype(F32)).astype(BF)
        out_ref[:, :, 0:Q] = put_last(total).reshape(E, 8, Q).astype(BF)
        products = (part_ref[...] + got_part_ref[...]).astype(BF).astype(F32)
        at = iota((E, 1152), 1)
        source = jnp.where(at < 1024, at % 512 // 8, (at - 1024) // 2)
        mine = jnp.where(source == iota((E, 1152), 0), products, 0.0).astype(BF)
        at = iota((1152, 128), 0)
        slot = jnp.where(at < 1024, at // 512 * 8 + at % 8, 16 + at % 2)
        table = dot(mine, ones_where(slot == iota((1152, 128), 1)).astype(BF)).astype(BF)
        place = ones_where(iota((F1, E), 0) == 8 * iota((F1, E), 1)).astype(BF)
        out_ref[:, :, Q:512] = dot(place, table).reshape(E, 8, 128).astype(BF)


def pack(mine, got, part, got_part):
    main = pl.BlockSpec((F1, 512), lambda b: (0, jnp.minimum(b, 2)))
    last = pl.BlockSpec((128, H), lambda b: (4, 0))
    line = pl.BlockSpec((1, 1152), lambda b: (0, 0))
    return pl.pallas_call(
        pack_kernel,
        grid=(4,),
        in_specs=[main, main, last, last, line, line],
        out_specs=pl.BlockSpec((E, 8, 512), lambda b: (0, 0, b)),
        out_shape=jax.ShapeDtypeStruct((E, 8, 2048), BF),
        name="pack",
    )(mine, got, mine, got, part, got_part)


def token_ranks_kernel(exp_ref, out_ref):
    exp = exp_ref[...]
    ids = iota((TOK, E), 1)
    named = ones_where(exp[:, 0:1] == ids) + ones_where(exp[:, 1:2] == ids)
    earlier = ones_where(iota((TOK, TOK), 1) < iota((TOK, TOK), 0)).astype(BF)
    ranks = jnp.where(named > 0.5, dot(earlier, named.astype(BF)), -1.0).astype(BF)
    spread = ones_where(iota((E, F1), 0) == iota((E, F1), 1) // 8).astype(BF)
    out_ref[...] = dot(ranks, spread)


def token_ranks(experts):
    return pl.pallas_call(
        token_ranks_kernel, out_shape=jax.ShapeDtypeStruct((TOK, F1), F32), name="token_ranks"
    )(experts)


def flat_rows(ref):
    return ref[...].astype(F32).reshape(F1, ref.shape[2]).astype(BF)


def column_slots(piece):
    i = iota((TOK, F1), 1) % 8
    return (16 + i % 2 if piece == 2 else i + 8 * piece).astype(F32)


def combine_one_kernel(ranks_ref, one_ref, out_ref):
    hit = ones_where(ranks_ref[...] == column_slots(0)).astype(BF)
    out_ref[...] = dot(hit, flat_rows(one_ref))


def combine_one(ranks, one):
    return pl.pallas_call(
        combine_one_kernel,
        grid=(4,),
        in_specs=[
            pl.BlockSpec((TOK, F1), lambda b: (0, 0)),
            pl.BlockSpec((E, 8, Q), lambda b: (0, 0, b)),
        ],
        out_specs=pl.BlockSpec((TOK, Q), lambda b: (0, b)),
        out_shape=jax.ShapeDtypeStruct((TOK, H), F32),
        name="combine_one",
    )(ranks, one)


def combine_two_kernel(ranks_ref, exp_ref, gate_ref, sum_ref, two_ref, last_ref, prod_ref, out_ref, gate_out_ref):
    b = pl.program_id(0)

    @pl.when(b == 0)
    def _():
        pick = ones_where(iota((E, F1), 1) == 8 * iota((E, F1), 0)).astype(BF)
        table = dot(pick, flat_rows(prod_ref)).astype(BF)
        for k in range(2):
            exp = exp_ref[:, k : k + 1]
            at = iota((TOK, F1), 1) == 8 * exp
            rank = jnp.sum(jnp.where(at, ranks_ref[...], 0.0), axis=1, keepdims=True)
            found = dot(ones_where(iota((TOK, E), 1) == exp).astype(BF), table)
            here = iota((TOK, 128), 1).astype(F32) == rank
            found = jnp.sum(jnp.where(here, found, 0.0), axis=1, keepdims=True)
            gate_out_ref[:, k : k + 1] = found / gate_ref[:, k : k + 1]

    ranks = ranks_ref[...]
    block = iota((TOK, F1), 1) % 8 // 2
    total = sum_ref[...] + dot(ones_where(ranks == column_slots(1)).astype(BF), flat_rows(two_ref))
    hit = (ranks == column_slots(2)) & (block == b)
    out_ref[...] = (total + dot(ones_where(hit).astype(BF), flat_rows(last_ref))).astype(BF)


def combine_two(ranks, experts, gate, total, two):
    small = pl.BlockSpec((TOK, 2), lambda b: (0, 0))
    return pl.pallas_call(
        combine_two_kernel,
        grid=(4,),
        in_specs=[
            pl.BlockSpec((TOK, F1), lambda b: (0, 0)),
            small,
            small,
            pl.BlockSpec((TOK, Q), lambda b: (0, b)),
            pl.BlockSpec((E, 8, Q), lambda b: (0, 0, b)),
            pl.BlockSpec((E, 8, Q), lambda b: (0, 0, 4)),
            pl.BlockSpec((E, 8, 128), lambda b: (0, 0, 15)),
        ],
        out_specs=[pl.BlockSpec((TOK, Q), lambda b: (0, b)), small],
        out_shape=[jax.ShapeDtypeStruct((TOK, H), BF), jax.ShapeDtypeStruct((TOK, 2), F32)],
        name="combine_two",
    )(ranks, experts, gate, total, two, two, two)


def weight_grads_kernel(x_ref, g1_ref, u1_ref, g2_ref, u2_ref, gate_ref, up_ref, norm_ref, turned_ref):
    @pl.when(pl.program_id(0) == 0)
    def _():
        for at, one_ref, two_ref in ((0, g1_ref, g2_ref), (384, u1_ref, u2_ref)):
            turned_ref[at : at + 384, 0:F1] = one_ref[...].T
            turned_ref[at : at + 384, F1:1152] = two_ref[...].T

    total = dot(turned_ref[...], x_ref[...])
    for k, ref in enumerate((gate_ref, up_ref)):
        part = total[384 * k : 384 * k + 384]
        norm_ref[k : k + 1, :] = jnp.sum(part * part, axis=0, keepdims=True)
        ref[...] = part.T.astype(BF)


def weight_grads(rows, g1, u1, g2, u2):
    def whole(a):
        return pl.BlockSpec(a.shape, lambda b: (0, 0))

    block = pl.BlockSpec((512, 384), lambda b: (b, 0))
    shape = jax.ShapeDtypeStruct((2 * H, 384), BF)
    return pl.pallas_call(
        weight_grads_kernel,
        grid=(6,),
        in_specs=[pl.BlockSpec((1152, 512), lambda b: (0, b)), whole(g1), whole(u1), whole(g2), whole(u2)],
        out_specs=[block, block, pl.BlockSpec((2, 512), lambda b: (0, b))],
        out_shape=[shape, shape, jax.ShapeDtypeStruct((2, 2 * H), F32)],
        scratch_shapes=[pltpu.VMEM((768, 1152), BF)],
        name="weight_grads",
    )(rows, g1, u1, g2, u2)


def to_experts(x):
    return lax.all_to_all(x, "ep", split_axis=0, concat_axis=0, tiled=True)


def swap_cores(x):
    return lax.ppermute(x, "tp", [(0, 1), (1, 0)])


def half(mat, index, axis):
    return lax.dynamic_slice_in_dim(mat, index * H, H, axis)


def step(tokens, cotangent, experts, gate, w_gate, w_up, w_down):
    core = lax.axis_index("tp").astype(jnp.int32)
    core_arg = core.reshape(1)
    gate_mat, up_mat, down_mat = w_gate[0], w_up[0], w_down[0]
    exp_t, gate_t = experts.T, gate.T
    gates = [half(gate_mat, index, 0) for index in (core, 1 - core)]
    ups = [half(up_mat, index, 0) for index in (core, 1 - core)]
    downs = [half(down_mat, index, 1) for index in (core, 1 - core)]
    tok_own, ranks, gates_of = send_tokens(exp_t, gate_t, tokens)
    tok_own = to_experts(tok_own)
    cot_one = send(ranks, gates_of, cotangent, 0, 4)
    cot_one = to_experts(cot_one)
    cot_two = send(ranks, gates_of, cotangent, 4, 9)
    by_token = token_ranks(experts)
    cot_two = to_experts(cot_two)
    tok_other = swap_cores(tok_own)

    rows_in = unpack(core_arg, tok_own, tok_other)
    gate_pre = dot(rows_in, gate_mat)
    up_pre = dot(rows_in, up_mat)
    sigma = jax.nn.sigmoid(gate_pre)
    active = gate_pre * sigma
    hidden = (active * up_pre).astype(BF)
    gate_slope = up_pre * sigma * (1.0 + gate_pre * (1.0 - sigma))

    def chunk(rows, lo, hi):
        grad = rows[0]
        for part in rows[1:]:
            grad = grad + part
        parts = jnp.sum(hidden[lo:hi].astype(F32) * grad, axis=1)
        gate_grad_pre = (grad * gate_slope[lo:hi]).astype(BF)
        up_grad_pre = (grad * active[lo:hi]).astype(BF)

        def partial(index):
            return (dot_last(gate_grad_pre, gates[index]) + dot_last(up_grad_pre, ups[index])).astype(BF)

        sent = swap_cores(partial(1))
        return parts, gate_grad_pre, up_grad_pre, partial(0), sent

    cot_one_other = swap_cores(cot_one)
    own = cot_one.reshape(F1, H)
    other = cot_one_other.reshape(F1, H)
    one = chunk((dot_last(own, downs[0]), dot_last(other, downs[1])), 0, F1)
    back_one = (one[3].astype(F32) + one[4].astype(F32)).astype(BF).reshape(E, 8, H)
    back_one = to_experts(back_one)

    cot_two_other = swap_cores(cot_two)
    rows_two = unpack(core_arg, cot_two, cot_two_other)
    two = chunk((dot_last(rows_two, down_mat),), F1, 1152)
    parts = jnp.concatenate([one[0], two[0]])
    parts = parts.reshape(1, 1152)
    back_two = pack(two[3], two[4], parts, swap_cores(parts))
    back_two = to_experts(back_two)

    down_own = dot_rows(hidden[:F1], own)
    down_other = dot_rows(hidden[:F1], other)
    gate_grad, up_grad, norms = weight_grads(rows_in, one[1], one[2], two[1], two[2])
    norms = norms + swap_cores(norms)
    down_one = jnp.where(
        core == 0,
        jnp.concatenate([down_own, down_other], axis=1),
        jnp.concatenate([down_other, down_own], axis=1),
    )
    down_sum = down_one + dot_rows(hidden[F1:], rows_two)
    down_norms = jnp.sum(down_sum * down_sum, axis=1)

    back_sum = combine_one(by_token, back_one)
    token_grad, gates_grad = combine_two(by_token, experts, gate, back_sum, back_two)
    return (
        token_grad,
        gates_grad,
        gate_grad[None],
        up_grad[None],
        down_sum.astype(BF)[None],
        norms[0:1],
        norms[1:2],
        down_norms[None],
    )


def solution(mesh):
    placed = (
        P("ep", "tp"),
        P("ep", "tp"),
        P("ep", None),
        P("ep", None),
        P("ep", None, "tp"),
        P("ep", None, "tp"),
        P("ep", "tp", None),
    )
    return jax.shard_map(
        step,
        mesh=mesh,
        in_specs=placed,
        out_specs=(
            P("ep", "tp"),
            P("ep", None),
            P("ep", None, "tp"),
            P("ep", None, "tp"),
            P("ep", "tp", None),
            P("ep", None),
            P("ep", None),
            P("ep", "tp"),
        ),
        check_vma=False,
    )
```

```python
import functools

import jax
import jax.numpy as jnp
from jax import lax
from jax.experimental import pallas as pl
from jax.experimental.pallas import tpu as pltpu
from jax.sharding import PartitionSpec as P


E = 64
TOK = 384
H = 1536
Q = 384
F1 = E * 8
BF = jnp.bfloat16
F32 = jnp.float32


def iota(shape, axis):
    return lax.broadcasted_iota(jnp.int32, shape, axis)


def dot(a, b):
    return lax.dot_general(a, b, (((1,), (0,)), ((), ())), preferred_element_type=F32)


def dot_last(a, b):
    return lax.dot_general(a, b, (((1,), (1,)), ((), ())), preferred_element_type=F32)


def dot_rows(a, b):
    return lax.dot_general(a, b, (((0,), (0,)), ((), ())), preferred_element_type=F32)


def ones_where(mask):
    return jnp.where(mask, 1.0, 0.0)


def named_by(exp):
    ids = iota((E, TOK), 0)
    return exp[0:1, :] == ids, exp[1:2, :] == ids


def slot_ranks(exp):
    first, second = named_by(exp)
    named = ones_where(first) + ones_where(second)
    earlier = ones_where(iota((TOK, TOK), 0) < iota((TOK, TOK), 1)).astype(BF)
    return named, dot(named.astype(BF), earlier)


def spread_rows(per_expert):
    spread = ones_where(iota((F1, E), 0) // 8 == iota((F1, E), 1)).astype(BF)
    return dot(spread, per_expert)


def row_slots(piece):
    i = iota((F1, TOK), 0) % 8
    return jnp.where(piece == 2, 16 + i % 2, i + 8 * piece).astype(F32)


def put_last(rows):
    row = iota((F1, 128), 0)
    col = iota((F1, 128), 1)
    total = jnp.zeros((F1, Q), F32)
    for q in range(4):
        place = ones_where(row == col // 2 * 8 + 2 * q + col % 2).astype(BF)
        total = total + dot(place, rows[:, q * Q : (q + 1) * Q])
    return total


def send_tokens_kernel(exp_ref, gate_ref, src_ref, out_ref, ranks_ref, gates_ref, line_ref, small_ref):
    b = pl.program_id(0)

    @pl.when(b == 0)
    def _():
        exp = exp_ref[...]
        named, ranks = slot_ranks(exp)
        small = jnp.where(named > 0.5, ranks, -1.0).astype(BF)
        small_ref[...] = small
        ranks_ref[...] = spread_rows(small)
        for k, mask in enumerate(named_by(exp)):
            line_ref[k : k + 1, :] = jnp.sum(jnp.where(mask, ranks, 0.0), axis=0, keepdims=True)

    def rows(piece, lo, hi):
        hit = ones_where(ranks_ref[...] == row_slots(jnp.int32(piece))).astype(BF)
        return dot(hit, src_ref[:, lo:hi]).reshape(E, 8, hi - lo).astype(BF)

    @pl.when(b == 0)
    def _():
        out_ref[...] = rows(0, 0, 1152)

    @pl.when(b == 1)
    def _():
        out_ref[:, :, 0:384] = rows(0, 1152, 1536)
        out_ref[:, :, 384:1152] = rows(1, 0, 768)

    @pl.when(b == 2)
    def _():
        out_ref[:, :, 0:768] = rows(1, 768, 1536)
        row = iota((128, E), 0)
        spread = ones_where(row // 2 == iota((128, E), 1)).astype(BF)
        slot = (16 + iota((128, TOK), 0) % 2).astype(F32)
        hit = ones_where(dot(spread, small_ref[...]) == slot).astype(BF)
        last = dot(hit, src_ref[...]).astype(BF)
        out_ref[:, :, 768:1152] = put_last(last).reshape(E, 8, Q).astype(BF)
        first, second = named_by(exp_ref[...])
        gate = gate_ref[...]
        rest = jnp.where(first, gate[0:1, :], 0.0) + jnp.where(second, gate[1:2, :], 0.0)
        total = jnp.zeros((F1, TOK), F32)
        for _ in range(3):
            part = rest.astype(BF)
            rest = rest - part.astype(F32)
            total = total + spread_rows(part)
        gates_ref[...] = total


def send_tokens(exp_t, gate_t, tokens):
    small = pl.BlockSpec((2, TOK), lambda b: (0, 0))
    table = pl.BlockSpec((F1, TOK), lambda b: (0, 0))
    shape = jax.ShapeDtypeStruct((F1, TOK), F32)
    return pl.pallas_call(
        send_tokens_kernel,
        grid=(3,),
        in_specs=[small, small, pl.BlockSpec((TOK, H), lambda b: (0, 0))],
        out_specs=[pl.BlockSpec((E, 8, 1152), lambda b: (0, 0, b)), table, table, small],
        out_shape=[
            jax.ShapeDtypeStruct((E, 8, 3456), BF),
            shape,
            shape,
            jax.ShapeDtypeStruct((2, TOK), F32),
        ],
        scratch_shapes=[pltpu.VMEM((E, TOK), BF)],
        name="send_tokens",
    )(exp_t, gate_t, tokens)


def send_kernel(lo, last, ranks_ref, gates_ref, src_ref, out_ref):
    b = pl.program_id(0) + lo

    def scaled(hit, rows):
        rows = rows * jnp.sum(jnp.where(hit, gates_ref[...], 0.0), axis=1, keepdims=True)
        return rows.reshape(E, 8, Q).astype(BF)

    @pl.when(b < 8)
    def _():
        hit = ranks_ref[...] == row_slots(b // 4)
        src = src_ref[:, pl.ds(pl.multiple_of((b % 4) * Q, Q), Q)]
        out_ref[...] = scaled(hit, dot(ones_where(hit).astype(BF), src))

    if last:

        @pl.when(b == 8)
        def _():
            hit = ranks_ref[...] == row_slots(jnp.int32(2))
            block = (iota((F1, TOK), 0) % 8) // 2
            total = jnp.zeros((F1, Q), F32)
            for q in range(4):
                pick = ones_where(hit & (block == q)).astype(BF)
                total = total + dot(pick, src_ref[:, q * Q : (q + 1) * Q])
            out_ref[...] = scaled(hit, total)


def send(ranks, gates, src, lo, hi):
    whole = pl.BlockSpec((F1, TOK), lambda b: (0, 0))
    return pl.pallas_call(
        functools.partial(send_kernel, lo, hi == 9),
        grid=(hi - lo,),
        in_specs=[whole, whole, pl.BlockSpec((TOK, H), lambda b: (0, 0))],
        out_specs=pl.BlockSpec((E, 8, Q), lambda b: (0, 0, b)),
        out_shape=jax.ShapeDtypeStruct((E, 8, (hi - lo) * Q), BF),
        name="send",
    )(ranks, gates, src)


def unpack_last(last):
    flat = last.astype(F32).reshape(F1, Q).astype(BF)
    row = iota((128, F1), 0)
    pieces = []
    for q in range(4):
        pick = ones_where(row // 2 * 8 + 2 * q + row % 2 == iota((128, F1), 1)).astype(BF)
        pieces.append(dot(pick, flat).astype(BF))
    return pieces


def fill_rows(steps, core_ref, own_ref, other_ref, own_last_ref, other_last_ref, rows_ref):
    b = pl.program_id(0)
    core = core_ref[0]
    sides = ((core, own_ref, own_last_ref), (1 - core, other_ref, other_last_ref))

    @pl.when(b < steps)
    def _():
        for half, part_ref, _ in sides:
            rows = part_ref[...].astype(F32).reshape(128, H).astype(BF)
            rows_ref[:, pl.ds(pl.multiple_of(half * H, H), H)] = rows

    @pl.when(b == steps)
    def _():
        for half, _, last_ref in sides:
            for q, piece in enumerate(unpack_last(last_ref[...])):
                rows_ref[:, pl.ds(pl.multiple_of(half * H + q * Q, Q), Q)] = piece


def packed_specs(wide):
    steps = 4 * wide

    def rows_at(b):
        bb = jnp.minimum(b, steps - 1)
        return (bb % 4, 0, bb // 4)

    rows = pl.BlockSpec((16, 8, H), rows_at)
    last = pl.BlockSpec((E, 8, Q), lambda b: (0, 0, wide * 4))
    return [pl.BlockSpec(memory_space=pltpu.SMEM), rows, rows, last, last]


def forward_kernel(core_ref, own_ref, other_ref, own_last_ref, other_last_ref, *refs):
    gate_ref, up_ref, rows_ref, hidden_ref, active_ref, slope_ref = refs
    fill_rows(8, core_ref, own_ref, other_ref, own_last_ref, other_last_ref, rows_ref)
    rows = rows_ref[...]
    gate_pre = dot(rows, gate_ref[...])
    up_pre = dot(rows, up_ref[...])
    sigma = jax.nn.sigmoid(gate_pre)
    active = gate_pre * sigma
    active_ref[...] = active
    hidden_ref[...] = (active * up_pre).astype(BF)
    slope_ref[...] = up_pre * sigma * (1.0 + gate_pre * (1.0 - sigma))


def forward(core, own, other, gate_mat, up_mat):
    weights = pl.BlockSpec((2 * H, Q), lambda b: (0, 0))
    block = pl.BlockSpec((128, Q), lambda b: (b, 0))
    return pl.pallas_call(
        forward_kernel,
        grid=(9,),
        in_specs=packed_specs(2) + [weights, weights],
        out_specs=[pl.BlockSpec((128, 2 * H), lambda b: (b, 0)), block, block, block],
        out_shape=[
            jax.ShapeDtypeStruct((1152, 2 * H), BF),
            jax.ShapeDtypeStruct((1152, Q), BF),
            jax.ShapeDtypeStruct((1152, Q), F32),
            jax.ShapeDtypeStruct((1152, Q), F32),
        ],
        name="forward",
    )(core, own, other, own, other, gate_mat, up_mat)


def middle_kernel(core_ref, own_ref, other_ref, own_last_ref, other_last_ref, *refs):
    down_ref, hidden_ref, active_ref, slope_ref, rows_ref, gate_ref, up_ref, part_ref = refs
    fill_rows(4, core_ref, own_ref, other_ref, own_last_ref, other_last_ref, rows_ref)
    grad = dot(rows_ref[...], down_ref[...])
    part = jnp.sum(hidden_ref[...].astype(F32) * grad, axis=1, keepdims=True)
    part_ref[...] = jnp.broadcast_to(part, (128, 128)).T[0:1, :]
    gate_ref[...] = (grad * slope_ref[...]).astype(BF)
    up_ref[...] = (grad * active_ref[...]).astype(BF)


def middle(core, own, other, down_turned, hidden, active, slope):
    late = pl.BlockSpec((128, Q), lambda b: (b + 4, 0))
    block = pl.BlockSpec((128, Q), lambda b: (b, 0))
    shape = jax.ShapeDtypeStruct((640, Q), BF)
    return pl.pallas_call(
        middle_kernel,
        grid=(5,),
        in_specs=packed_specs(1) + [pl.BlockSpec((2 * H, Q), lambda b: (0, 0)), late, late, late],
        out_specs=[
            pl.BlockSpec((128, 2 * H), lambda b: (b, 0)),
            block,
            block,
            pl.BlockSpec((1, 128), lambda b: (0, b)),
        ],
        out_shape=[
            jax.ShapeDtypeStruct((640, 2 * H), BF),
            shape,
            shape,
            jax.ShapeDtypeStruct((1, 640), F32),
        ],
        name="middle",
    )(core, own, other, own, other, down_turned, hidden, active, slope)


def pack_kernel(mine_ref, got_ref, mine_last_ref, got_last_ref, part_ref, got_part_ref, out_ref):
    b = pl.program_id(0)

    @pl.when(b < 3)
    def _():
        total = mine_ref[...].astype(F32) + got_ref[...].astype(F32)
        out_ref[...] = total.reshape(E, 8, 512).astype(BF)

    @pl.when(b == 3)
    def _():
        total = (mine_last_ref[...].astype(F32) + got_last_ref[...].astype(F32)).astype(BF)
        out_ref[:, :, 0:Q] = put_last(total).reshape(E, 8, Q).astype(BF)
        products = (part_ref[...] + got_part_ref[...]).astype(BF).astype(F32)
        at = iota((E, 1152), 1)
        source = jnp.where(at < 1024, at % 512 // 8, (at - 1024) // 2)
        mine = jnp.where(source == iota((E, 1152), 0), products, 0.0).astype(BF)
        at = iota((1152, 128), 0)
        slot = jnp.where(at < 1024, at // 512 * 8 + at % 8, 16 + at % 2)
        table = dot(mine, ones_where(slot == iota((1152, 128), 1)).astype(BF)).astype(BF)
        place = ones_where(iota((F1, E), 0) == 8 * iota((F1, E), 1)).astype(BF)
        out_ref[:, :, Q:512] = dot(place, table).reshape(E, 8, 128).astype(BF)


def pack(mine, got, part, got_part):
    main = pl.BlockSpec((F1, 512), lambda b: (0, jnp.minimum(b, 2)))
    last = pl.BlockSpec((128, H), lambda b: (4, 0))
    line = pl.BlockSpec((1, 1152), lambda b: (0, 0))
    return pl.pallas_call(
        pack_kernel,
        grid=(4,),
        in_specs=[main, main, last, last, line, line],
        out_specs=pl.BlockSpec((E, 8, 512), lambda b: (0, 0, b)),
        out_shape=jax.ShapeDtypeStruct((E, 8, 2048), BF),
        name="pack",
    )(mine, got, mine, got, part, got_part)


def token_ranks_kernel(exp_ref, out_ref):
    exp = exp_ref[...]
    ids = iota((TOK, E), 1)
    named = ones_where(exp[:, 0:1] == ids) + ones_where(exp[:, 1:2] == ids)
    earlier = ones_where(iota((TOK, TOK), 1) < iota((TOK, TOK), 0)).astype(BF)
    ranks = jnp.where(named > 0.5, dot(earlier, named.astype(BF)), -1.0).astype(BF)
    spread = ones_where(iota((E, F1), 0) == iota((E, F1), 1) // 8).astype(BF)
    out_ref[...] = dot(ranks, spread)


def token_ranks(experts):
    return pl.pallas_call(
        token_ranks_kernel, out_shape=jax.ShapeDtypeStruct((TOK, F1), F32), name="token_ranks"
    )(experts)


def flat_rows(ref):
    return ref[...].astype(F32).reshape(F1, ref.shape[2]).astype(BF)


def column_slots(piece):
    i = iota((TOK, F1), 1) % 8
    return (16 + i % 2 if piece == 2 else i + 8 * piece).astype(F32)


def combine_one_kernel(ranks_ref, one_ref, out_ref):
    hit = ones_where(ranks_ref[...] == column_slots(0)).astype(BF)
    out_ref[...] = dot(hit, flat_rows(one_ref))


def combine_one(ranks, one):
    return pl.pallas_call(
        combine_one_kernel,
        grid=(2,),
        in_specs=[
            pl.BlockSpec((TOK, F1), lambda b: (0, 0)),
            pl.BlockSpec((E, 8, 2 * Q), lambda b: (0, 0, b)),
        ],
        out_specs=pl.BlockSpec((TOK, 2 * Q), lambda b: (0, b)),
        out_shape=jax.ShapeDtypeStruct((TOK, H), F32),
        name="combine_one",
    )(ranks, one)


def combine_two_kernel(ranks_ref, line_ref, exp_ref, gate_ref, *refs):
    sum_ref, two_ref, last_ref, prod_ref, out_ref, gate_out_ref = refs
    b = pl.program_id(0)

    @pl.when(b == 0)
    def _():
        pick = ones_where(iota((E, F1), 1) == 8 * iota((E, F1), 0)).astype(BF)
        table = dot(pick, flat_rows(prod_ref)).astype(BF)
        for k in range(2):
            named = ones_where(iota((E, TOK), 0) == exp_ref[k : k + 1, :]).astype(BF)
            found = dot_rows(table, named)
            here = iota((128, TOK), 0).astype(F32) == line_ref[k : k + 1, :]
            found = jnp.sum(jnp.where(here, found, 0.0), axis=0, keepdims=True)
            gate_out_ref[k : k + 1, :] = found / gate_ref[k : k + 1, :]

    ranks = ranks_ref[...]
    block = iota((TOK, F1), 1) % 8 // 2
    total = sum_ref[...] + dot(ones_where(ranks == column_slots(1)).astype(BF), flat_rows(two_ref))
    hit = (ranks == column_slots(2)) & (block == b)
    out_ref[...] = (total + dot(ones_where(hit).astype(BF), flat_rows(last_ref))).astype(BF)


def combine_two(ranks, lines, exp_t, gate_t, total, two):
    small = pl.BlockSpec((2, TOK), lambda b: (0, 0))
    return pl.pallas_call(
        combine_two_kernel,
        grid=(4,),
        in_specs=[
            pl.BlockSpec((TOK, F1), lambda b: (0, 0)),
            small,
            small,
            small,
            pl.BlockSpec((TOK, Q), lambda b: (0, b)),
            pl.BlockSpec((E, 8, Q), lambda b: (0, 0, b)),
            pl.BlockSpec((E, 8, Q), lambda b: (0, 0, 4)),
            pl.BlockSpec((E, 8, 128), lambda b: (0, 0, 15)),
        ],
        out_specs=[pl.BlockSpec((TOK, Q), lambda b: (0, b)), small],
        out_shape=[jax.ShapeDtypeStruct((TOK, H), BF), jax.ShapeDtypeStruct((2, TOK), F32)],
        name="combine_two",
    )(ranks, lines, exp_t, gate_t, total, two, two, two)


def turn_kernel(src_ref, out_ref):
    out_ref[...] = src_ref[...].T


def turn(mat):
    return pl.pallas_call(
        turn_kernel,
        grid=(6,),
        in_specs=[pl.BlockSpec((Q, 512), lambda b: (0, b))],
        out_specs=pl.BlockSpec((512, Q), lambda b: (b, 0)),
        out_shape=jax.ShapeDtypeStruct((2 * H, Q), BF),
        name="turn",
    )(mat)


def weight_grads_kernel(x_ref, g1_ref, u1_ref, g2_ref, u2_ref, gate_ref, up_ref, norm_ref, turned_ref):
    @pl.when(pl.program_id(0) == 0)
    def _():
        for at, one_ref, two_ref in ((0, g1_ref, g2_ref), (384, u1_ref, u2_ref)):
            turned_ref[at : at + 384, 0:F1] = one_ref[...].T
            turned_ref[at : at + 384, F1:1152] = two_ref[...].T

    total = dot(turned_ref[...], x_ref[...])
    for k, ref in enumerate((gate_ref, up_ref)):
        part = total[384 * k : 384 * k + 384]
        norm_ref[k : k + 1, :] = jnp.sum(part * part, axis=0, keepdims=True)
        ref[...] = part.T.astype(BF)


def weight_grads(rows, g1, u1, g2, u2):
    def whole(a):
        return pl.BlockSpec(a.shape, lambda b: (0, 0))

    block = pl.BlockSpec((512, 384), lambda b: (b, 0))
    shape = jax.ShapeDtypeStruct((2 * H, 384), BF)
    return pl.pallas_call(
        weight_grads_kernel,
        grid=(6,),
        in_specs=[pl.BlockSpec((1152, 512), lambda b: (0, b)), whole(g1), whole(u1), whole(g2), whole(u2)],
        out_specs=[block, block, pl.BlockSpec((2, 512), lambda b: (0, b))],
        out_shape=[shape, shape, jax.ShapeDtypeStruct((2, 2 * H), F32)],
        scratch_shapes=[pltpu.VMEM((768, 1152), BF)],
        name="weight_grads",
    )(rows, g1, u1, g2, u2)


def to_experts(x):
    return lax.all_to_all(x, "ep", split_axis=0, concat_axis=0, tiled=True)


def swap_cores(x):
    return lax.ppermute(x, "tp", [(0, 1), (1, 0)])


def half(mat, index, axis):
    return lax.dynamic_slice_in_dim(mat, index * H, H, axis)


def step(tokens, cotangent, experts, gate, w_gate, w_up, w_down):
    core = lax.axis_index("tp").astype(jnp.int32)
    core_arg = core.reshape(1)
    gate_mat, up_mat, down_mat = w_gate[0], w_up[0], w_down[0]
    exp_t, gate_t = experts.T, gate.T
    gates = [half(gate_mat, index, 0) for index in (core, 1 - core)]
    ups = [half(up_mat, index, 0) for index in (core, 1 - core)]
    downs = [half(down_mat, index, 1) for index in (core, 1 - core)]
    down_turned = turn(down_mat)
    tok_own, ranks, gates_of, lines = send_tokens(exp_t, gate_t, tokens)
    tok_own = to_experts(tok_own)
    cot_one = send(ranks, gates_of, cotangent, 0, 4)
    cot_one = to_experts(cot_one)
    cot_two = send(ranks, gates_of, cotangent, 4, 9)
    by_token = token_ranks(experts)
    cot_two = to_experts(cot_two)
    tok_other = swap_cores(tok_own)

    rows_in, hidden, active, gate_slope = forward(core_arg, tok_own, tok_other, gate_mat, up_mat)

    def send_back(gate_grad_pre, up_grad_pre):
        def partial(index):
            return (dot_last(gate_grad_pre, gates[index]) + dot_last(up_grad_pre, ups[index])).astype(BF)

        sent = swap_cores(partial(1))
        return partial(0), sent

    cot_one_other = swap_cores(cot_one)
    own = cot_one.reshape(F1, H)
    other = cot_one_other.reshape(F1, H)
    grad = dot_last(own, downs[0]) + dot_last(other, downs[1])
    parts_one = jnp.sum(hidden[:F1].astype(F32) * grad, axis=1)
    gate_one = (grad * gate_slope[:F1]).astype(BF)
    up_one = (grad * active[:F1]).astype(BF)
    mine, sent = send_back(gate_one, up_one)
    back_one = (mine.astype(F32) + sent.astype(F32)).astype(BF).reshape(E, 8, H)
    back_one = to_experts(back_one)

    cot_two_other = swap_cores(cot_two)
    rows_two, gate_two, up_two, parts_two = middle(
        core_arg, cot_two, cot_two_other, down_turned, hidden, active, gate_slope
    )
    mine, sent = send_back(gate_two, up_two)
    parts = jnp.concatenate([parts_one.reshape(1, F1), parts_two], axis=1)
    back_two = pack(mine, sent, parts, swap_cores(parts))
    back_two = to_experts(back_two)

    down_own = dot_rows(hidden[:F1], own)
    down_other = dot_rows(hidden[:F1], other)
    gate_grad, up_grad, norms = weight_grads(rows_in, gate_one, up_one, gate_two, up_two)
    norms = norms + swap_cores(norms)
    down_one = jnp.where(
        core == 0,
        jnp.concatenate([down_own, down_other], axis=1),
        jnp.concatenate([down_other, down_own], axis=1),
    )
    down_sum = down_one + dot_rows(hidden[F1:], rows_two)
    down_norms = jnp.sum(down_sum * down_sum, axis=1)

    back_sum = combine_one(by_token, back_one)
    token_grad, gates_grad = combine_two(by_token, lines, exp_t, gate_t, back_sum, back_two)
    return (
        token_grad,
        gates_grad.T,
        gate_grad[None],
        up_grad[None],
        down_sum.astype(BF)[None],
        norms[0:1],
        norms[1:2],
        down_norms[None],
    )


def solution(mesh):
    placed = (
        P("ep", "tp"),
        P("ep", "tp"),
        P("ep", None),
        P("ep", None),
        P("ep", None, "tp"),
        P("ep", None, "tp"),
        P("ep", "tp", None),
    )
    return jax.shard_map(
        step,
        mesh=mesh,
        in_specs=placed,
        out_specs=(
            P("ep", "tp"),
            P("ep", None),
            P("ep", None, "tp"),
            P("ep", None, "tp"),
            P("ep", "tp", None),
            P("ep", None),
            P("ep", None),
            P("ep", "tp"),
        ),
        check_vma=False,
    )
```

```python
import functools

import jax
import jax.numpy as jnp
from jax import lax
from jax.experimental import pallas as pl
from jax.experimental.pallas import tpu as pltpu
from jax.sharding import PartitionSpec as P


E = 64
TOK = 384
H = 1536
Q = 384
F1 = E * 8
BF = jnp.bfloat16
F32 = jnp.float32


def iota(shape, axis):
    return lax.broadcasted_iota(jnp.int32, shape, axis)


def dot(a, b):
    return lax.dot_general(a, b, (((1,), (0,)), ((), ())), preferred_element_type=F32)


def dot_last(a, b):
    return lax.dot_general(a, b, (((1,), (1,)), ((), ())), preferred_element_type=F32)


def dot_rows(a, b):
    return lax.dot_general(a, b, (((0,), (0,)), ((), ())), preferred_element_type=F32)


def ones_where(mask):
    return jnp.where(mask, 1.0, 0.0)


def named_by(exp):
    ids = iota((E, TOK), 0)
    return exp[0:1, :] == ids, exp[1:2, :] == ids


def slot_ranks(exp):
    first, second = named_by(exp)
    named = ones_where(first) + ones_where(second)
    earlier = ones_where(iota((TOK, TOK), 0) < iota((TOK, TOK), 1)).astype(BF)
    return named, dot(named.astype(BF), earlier)


def spread_rows(per_expert):
    spread = ones_where(iota((F1, E), 0) // 8 == iota((F1, E), 1)).astype(BF)
    return dot(spread, per_expert)


def row_slots(piece):
    i = iota((F1, TOK), 0) % 8
    return jnp.where(piece == 2, 16 + i % 2, i + 8 * piece).astype(F32)


def put_last(rows):
    row = iota((F1, 128), 0)
    col = iota((F1, 128), 1)
    total = jnp.zeros((F1, Q), F32)
    for q in range(4):
        place = ones_where(row == col // 2 * 8 + 2 * q + col % 2).astype(BF)
        total = total + dot(place, rows[:, q * Q : (q + 1) * Q])
    return total


def send_first_kernel(exp_ref, gate_ref, tok_ref, cot_ref, out_ref, ranks_ref, gates_ref, line_ref, small_ref):
    b = pl.program_id(0)

    @pl.when(b == 0)
    def _():
        exp = exp_ref[...]
        first, second = named_by(exp)
        named, ranks = slot_ranks(exp)
        small = jnp.where(named > 0.5, ranks, -1.0).astype(BF)
        small_ref[...] = small
        ranks_ref[...] = spread_rows(small)
        for k, mask in enumerate((first, second)):
            line_ref[k : k + 1, :] = jnp.sum(jnp.where(mask, ranks, 0.0), axis=0, keepdims=True)
        gate = gate_ref[...]
        rest = jnp.where(first, gate[0:1, :], 0.0) + jnp.where(second, gate[1:2, :], 0.0)
        total = jnp.zeros((F1, TOK), F32)
        for _ in range(3):
            part = rest.astype(BF)
            rest = rest - part.astype(F32)
            total = total + spread_rows(part)
        gates_ref[...] = total

    def rows(piece, lo, hi):
        hit = ones_where(ranks_ref[...] == row_slots(jnp.int32(piece))).astype(BF)
        return dot(hit, tok_ref[:, lo:hi]).reshape(E, 8, hi - lo).astype(BF)

    @pl.when(b == 0)
    def _():
        hit = ranks_ref[...] == row_slots(jnp.int32(0))
        scale = jnp.sum(jnp.where(hit, gates_ref[...], 0.0), axis=1, keepdims=True)
        scaled = dot(ones_where(hit).astype(BF), cot_ref[...]) * scale
        out_ref[:, :, 0:H] = scaled.reshape(E, 8, H).astype(BF)
        out_ref[:, :, H:1664] = rows(0, 0, 128)

    @pl.when(b == 1)
    def _():
        out_ref[:, :, 0:1408] = rows(0, 128, H)
        out_ref[:, :, 1408:1664] = rows(1, 0, 256)

    @pl.when(b == 2)
    def _():
        out_ref[:, :, 0:1280] = rows(1, 256, H)
        row = iota((128, E), 0)
        spread = ones_where(row // 2 == iota((128, E), 1)).astype(BF)
        slot = (16 + iota((128, TOK), 0) % 2).astype(F32)
        hit = ones_where(dot(spread, small_ref[...]) == slot).astype(BF)
        last = dot(hit, tok_ref[...]).astype(BF)
        out_ref[:, :, 1280:1664] = put_last(last).reshape(E, 8, Q).astype(BF)


def send_first(exp_t, gate_t, tokens, cotangent):
    small = pl.BlockSpec((2, TOK), lambda b: (0, 0))
    table = pl.BlockSpec((F1, TOK), lambda b: (0, 0))
    source = pl.BlockSpec((TOK, H), lambda b: (0, 0))
    shape = jax.ShapeDtypeStruct((F1, TOK), F32)
    return pl.pallas_call(
        send_first_kernel,
        grid=(3,),
        in_specs=[small, small, source, source],
        out_specs=[pl.BlockSpec((E, 8, 1664), lambda b: (0, 0, b)), table, table, small],
        out_shape=[
            jax.ShapeDtypeStruct((E, 8, 4992), BF),
            shape,
            shape,
            jax.ShapeDtypeStruct((2, TOK), F32),
        ],
        scratch_shapes=[pltpu.VMEM((E, TOK), BF)],
        name="send_first",
    )(exp_t, gate_t, tokens, cotangent)


def send_kernel(lo, last, ranks_ref, gates_ref, src_ref, out_ref):
    b = pl.program_id(0) + lo

    def scaled(hit, rows):
        rows = rows * jnp.sum(jnp.where(hit, gates_ref[...], 0.0), axis=1, keepdims=True)
        return rows.reshape(E, 8, Q).astype(BF)

    @pl.when(b < 8)
    def _():
        hit = ranks_ref[...] == row_slots(b // 4)
        src = src_ref[:, pl.ds(pl.multiple_of((b % 4) * Q, Q), Q)]
        out_ref[...] = scaled(hit, dot(ones_where(hit).astype(BF), src))

    if last:

        @pl.when(b == 8)
        def _():
            hit = ranks_ref[...] == row_slots(jnp.int32(2))
            block = (iota((F1, TOK), 0) % 8) // 2
            total = jnp.zeros((F1, Q), F32)
            for q in range(4):
                pick = ones_where(hit & (block == q)).astype(BF)
                total = total + dot(pick, src_ref[:, q * Q : (q + 1) * Q])
            out_ref[...] = scaled(hit, total)


def send(ranks, gates, src, lo, hi):
    whole = pl.BlockSpec((F1, TOK), lambda b: (0, 0))
    return pl.pallas_call(
        functools.partial(send_kernel, lo, hi == 9),
        grid=(hi - lo,),
        in_specs=[whole, whole, pl.BlockSpec((TOK, H), lambda b: (0, 0))],
        out_specs=pl.BlockSpec((E, 8, Q), lambda b: (0, 0, b)),
        out_shape=jax.ShapeDtypeStruct((E, 8, (hi - lo) * Q), BF),
        name="send",
    )(ranks, gates, src)


def unpack_last(last):
    flat = last.astype(F32).reshape(F1, Q).astype(BF)
    row = iota((128, F1), 0)
    pieces = []
    for q in range(4):
        pick = ones_where(row // 2 * 8 + 2 * q + row % 2 == iota((128, F1), 1)).astype(BF)
        pieces.append(dot(pick, flat).astype(BF))
    return pieces


def fill_rows(steps, core_ref, parts, rows_ref):
    b = pl.program_id(0)
    core = core_ref[0]
    halves = (core, 1 - core)

    @pl.when(b < steps)
    def _():
        for half, part_ref in zip(halves, parts[:2]):
            rows = part_ref[...].astype(F32).reshape(128, H).astype(BF)
            rows_ref[:, pl.ds(pl.multiple_of(half * H, H), H)] = rows

    if len(parts) == 4:

        @pl.when(b == steps)
        def _():
            for half, last_ref in zip(halves, parts[2:]):
                for q, piece in enumerate(unpack_last(last_ref[...])):
                    rows_ref[:, pl.ds(pl.multiple_of(half * H + q * Q, Q), Q)] = piece


def packed_specs(start, wide, last_at):
    steps = 4 * wide

    def rows_at(b):
        bb = jnp.minimum(b, steps - 1)
        return (bb % 4, 0, start + bb // 4)

    rows = pl.BlockSpec((16, 8, H), rows_at)
    last = pl.BlockSpec((E, 8, Q), lambda b: (0, 0, last_at))
    specs = [pl.BlockSpec(memory_space=pltpu.SMEM), rows, rows]
    return specs + [last, last] if last_at else specs


def forward_kernel(core_ref, own_ref, other_ref, own_last_ref, other_last_ref, *refs):
    gate_ref, up_ref, rows_ref, hidden_ref, active_ref, slope_ref = refs
    fill_rows(8, core_ref, (own_ref, other_ref, own_last_ref, other_last_ref), rows_ref)
    rows = rows_ref[...]
    gate_pre = dot(rows, gate_ref[...])
    up_pre = dot(rows, up_ref[...])
    sigma = jax.nn.sigmoid(gate_pre)
    active = gate_pre * sigma
    active_ref[...] = active
    hidden_ref[...] = (active * up_pre).astype(BF)
    slope_ref[...] = up_pre * sigma * (1.0 + gate_pre * (1.0 - sigma))


def forward(core, own, other, gate_mat, up_mat):
    weights = pl.BlockSpec((2 * H, Q), lambda b: (0, 0))
    block = pl.BlockSpec((128, Q), lambda b: (b, 0))
    return pl.pallas_call(
        forward_kernel,
        grid=(9,),
        in_specs=packed_specs(1, 2, 12) + [weights, weights],
        out_specs=[pl.BlockSpec((128, 2 * H), lambda b: (b, 0)), block, block, block],
        out_shape=[
            jax.ShapeDtypeStruct((1152, 2 * H), BF),
            jax.ShapeDtypeStruct((1152, Q), BF),
            jax.ShapeDtypeStruct((1152, Q), F32),
            jax.ShapeDtypeStruct((1152, Q), F32),
        ],
        name="forward",
    )(core, own, other, own, other, gate_mat, up_mat)


def middle_kernel(core_ref, *refs):
    down_ref, back_ref, hidden_ref, active_ref, slope_ref = refs[-10:-5]
    rows_ref, gate_ref, up_ref, part_ref, sent_ref = refs[-5:]
    fill_rows(4, core_ref, refs[:-10], rows_ref)
    grad = dot(rows_ref[...], down_ref[...])
    part = jnp.sum(hidden_ref[...].astype(F32) * grad, axis=1, keepdims=True)
    part_ref[...] = jnp.broadcast_to(part, (128, 128)).T[0:1, :]
    gate = (grad * slope_ref[...]).astype(BF)
    up = (grad * active_ref[...]).astype(BF)
    gate_ref[...] = gate
    up_ref[...] = up
    sent_ref[...] = dot(jnp.concatenate([gate, up], axis=1), back_ref[...]).astype(BF)


def middle(core, own, other, down_turned, back_turned, hidden, active, slope, lo, last):
    taken = pl.BlockSpec((128, Q), lambda b: (b + lo, 0))
    block = pl.BlockSpec((128, Q), lambda b: (b, 0))
    steps = 5 if last else 4
    shape = jax.ShapeDtypeStruct((128 * steps, Q), BF)
    sides = (own, other, own, other) if last else (own, other)
    return pl.pallas_call(
        middle_kernel,
        grid=(steps,),
        in_specs=packed_specs(0, 1, 4 if last else 0)
        + [
            pl.BlockSpec((2 * H, Q), lambda b: (0, 0)),
            pl.BlockSpec((2 * Q, H), lambda b: (0, 0)),
            taken,
            taken,
            taken,
        ],
        out_specs=[
            pl.BlockSpec((128, 2 * H), lambda b: (b, 0)),
            block,
            block,
            pl.BlockSpec((1, 128), lambda b: (0, b)),
            pl.BlockSpec((128, H), lambda b: (b, 0)),
        ],
        out_shape=[
            jax.ShapeDtypeStruct((128 * steps, 2 * H), BF),
            shape,
            shape,
            jax.ShapeDtypeStruct((1, 128 * steps), F32),
            jax.ShapeDtypeStruct((128 * steps, H), BF),
        ],
        name="middle",
    )(core, *sides, down_turned, back_turned, hidden, active, slope)


def pack_kernel(mine_ref, got_ref, mine_last_ref, got_last_ref, part_ref, got_part_ref, out_ref):
    b = pl.program_id(0)

    @pl.when(b < 3)
    def _():
        total = mine_ref[...].astype(F32) + got_ref[...].astype(F32)
        out_ref[...] = total.reshape(E, 8, 512).astype(BF)

    @pl.when(b == 3)
    def _():
        total = (mine_last_ref[...].astype(F32) + got_last_ref[...].astype(F32)).astype(BF)
        out_ref[:, :, 0:Q] = put_last(total).reshape(E, 8, Q).astype(BF)
        products = (part_ref[...] + got_part_ref[...]).astype(BF).astype(F32)
        at = iota((E, 1152), 1)
        source = jnp.where(at < 1024, at % 512 // 8, (at - 1024) // 2)
        mine = jnp.where(source == iota((E, 1152), 0), products, 0.0).astype(BF)
        at = iota((1152, 128), 0)
        slot = jnp.where(at < 1024, at // 512 * 8 + at % 8, 16 + at % 2)
        table = dot(mine, ones_where(slot == iota((1152, 128), 1)).astype(BF)).astype(BF)
        place = ones_where(iota((F1, E), 0) == 8 * iota((F1, E), 1)).astype(BF)
        out_ref[:, :, Q:512] = dot(place, table).reshape(E, 8, 128).astype(BF)


def pack(mine, got, part, got_part):
    main = pl.BlockSpec((F1, 512), lambda b: (0, jnp.minimum(b, 2)))
    last = pl.BlockSpec((128, H), lambda b: (4, 0))
    line = pl.BlockSpec((1, 1152), lambda b: (0, 0))
    return pl.pallas_call(
        pack_kernel,
        grid=(4,),
        in_specs=[main, main, last, last, line, line],
        out_specs=pl.BlockSpec((E, 8, 512), lambda b: (0, 0, b)),
        out_shape=jax.ShapeDtypeStruct((E, 8, 2048), BF),
        name="pack",
    )(mine, got, mine, got, part, got_part)


def token_ranks_kernel(exp_ref, out_ref):
    exp = exp_ref[...]
    ids = iota((TOK, E), 1)
    named = ones_where(exp[:, 0:1] == ids) + ones_where(exp[:, 1:2] == ids)
    earlier = ones_where(iota((TOK, TOK), 1) < iota((TOK, TOK), 0)).astype(BF)
    ranks = jnp.where(named > 0.5, dot(earlier, named.astype(BF)), -1.0).astype(BF)
    spread = ones_where(iota((E, F1), 0) == iota((E, F1), 1) // 8).astype(BF)
    out_ref[...] = dot(ranks, spread)


def token_ranks(experts):
    return pl.pallas_call(
        token_ranks_kernel, out_shape=jax.ShapeDtypeStruct((TOK, F1), F32), name="token_ranks"
    )(experts)


def flat_rows(ref):
    return ref[...].astype(F32).reshape(F1, ref.shape[2]).astype(BF)


def column_slots(piece):
    i = iota((TOK, F1), 1) % 8
    return (16 + i % 2 if piece == 2 else i + 8 * piece).astype(F32)


def combine_one_kernel(ranks_ref, one_ref, out_ref):
    hit = ones_where(ranks_ref[...] == column_slots(0)).astype(BF)
    out_ref[...] = dot(hit, flat_rows(one_ref))


def combine_one(ranks, one):
    return pl.pallas_call(
        combine_one_kernel,
        grid=(2,),
        in_specs=[
            pl.BlockSpec((TOK, F1), lambda b: (0, 0)),
            pl.BlockSpec((E, 8, 2 * Q), lambda b: (0, 0, b)),
        ],
        out_specs=pl.BlockSpec((TOK, 2 * Q), lambda b: (0, b)),
        out_shape=jax.ShapeDtypeStruct((TOK, H), F32),
        name="combine_one",
    )(ranks, one)


def combine_two_kernel(ranks_ref, line_ref, exp_ref, gate_ref, *refs):
    sum_ref, two_ref, last_ref, prod_ref, out_ref, gate_out_ref = refs
    b = pl.program_id(0)

    @pl.when(b == 0)
    def _():
        pick = ones_where(iota((E, F1), 1) == 8 * iota((E, F1), 0)).astype(BF)
        table = dot(pick, flat_rows(prod_ref)).astype(BF)
        for k in range(2):
            named = ones_where(iota((E, TOK), 0) == exp_ref[k : k + 1, :]).astype(BF)
            found = dot_rows(table, named)
            here = iota((128, TOK), 0).astype(F32) == line_ref[k : k + 1, :]
            found = jnp.sum(jnp.where(here, found, 0.0), axis=0, keepdims=True)
            gate_out_ref[k : k + 1, :] = found / gate_ref[k : k + 1, :]

    ranks = ranks_ref[...]
    block = iota((TOK, F1), 1) % 8 // 2
    total = sum_ref[...] + dot(ones_where(ranks == column_slots(1)).astype(BF), flat_rows(two_ref))
    hit = (ranks == column_slots(2)) & (block == b)
    out_ref[...] = (total + dot(ones_where(hit).astype(BF), flat_rows(last_ref))).astype(BF)


def combine_two(ranks, lines, exp_t, gate_t, total, two):
    small = pl.BlockSpec((2, TOK), lambda b: (0, 0))
    return pl.pallas_call(
        combine_two_kernel,
        grid=(4,),
        in_specs=[
            pl.BlockSpec((TOK, F1), lambda b: (0, 0)),
            small,
            small,
            small,
            pl.BlockSpec((TOK, Q), lambda b: (0, b)),
            pl.BlockSpec((E, 8, Q), lambda b: (0, 0, b)),
            pl.BlockSpec((E, 8, Q), lambda b: (0, 0, 4)),
            pl.BlockSpec((E, 8, 128), lambda b: (0, 0, 15)),
        ],
        out_specs=[pl.BlockSpec((TOK, Q), lambda b: (0, b)), small],
        out_shape=[jax.ShapeDtypeStruct((TOK, H), BF), jax.ShapeDtypeStruct((2, TOK), F32)],
        name="combine_two",
    )(ranks, lines, exp_t, gate_t, total, two, two, two)


def down_grads_kernel(hidden_ref, one_ref, two_ref, out_ref, norm_ref, turned_ref, sums_ref):
    b = pl.program_id(0)

    @pl.when(b == 0)
    def _():
        turned_ref[...] = hidden_ref[...].T
        sums_ref[...] = jnp.zeros((Q, 128), F32)

    total = dot(turned_ref[:, 0:F1], one_ref[...]) + dot(turned_ref[:, F1:1152], two_ref[...])
    out_ref[...] = total.astype(BF)
    sums_ref[...] += jnp.broadcast_to(jnp.sum(total * total, axis=1, keepdims=True), (Q, 128))

    @pl.when(b == 5)
    def _():
        norm_ref[...] = sums_ref[...].T[0:1, :]


def down_grads(hidden, one, two):
    return pl.pallas_call(
        down_grads_kernel,
        grid=(6,),
        in_specs=[
            pl.BlockSpec((1152, Q), lambda b: (0, 0)),
            pl.BlockSpec((F1, 512), lambda b: (0, b)),
            pl.BlockSpec((640, 512), lambda b: (0, b)),
        ],
        out_specs=[pl.BlockSpec((Q, 512), lambda b: (0, b)), pl.BlockSpec((1, Q), lambda b: (0, 0))],
        out_shape=[jax.ShapeDtypeStruct((Q, 2 * H), BF), jax.ShapeDtypeStruct((1, Q), F32)],
        scratch_shapes=[pltpu.VMEM((Q, 1152), BF), pltpu.VMEM((Q, 128), F32)],
        name="down_grads",
    )(hidden, one, two)


def turn_kernel(src_ref, out_ref):
    out_ref[...] = src_ref[...].T


def turn(mat):
    return pl.pallas_call(
        turn_kernel,
        grid=(6,),
        in_specs=[pl.BlockSpec((Q, 512), lambda b: (0, b))],
        out_specs=pl.BlockSpec((512, Q), lambda b: (b, 0)),
        out_shape=jax.ShapeDtypeStruct((2 * H, Q), BF),
        name="turn",
    )(mat)


def turn_back_kernel(core_ref, gate_ref, up_ref, out_ref):
    out_ref[0:Q, :] = gate_ref[...].T
    out_ref[Q : 2 * Q, :] = up_ref[...].T


def turn_back(core, gate_mat, up_mat):
    block = pl.BlockSpec((512, Q), lambda b, c: (3 * (1 - c[0]) + b, 0))
    return pl.pallas_call(
        turn_back_kernel,
        grid_spec=pltpu.PrefetchScalarGridSpec(
            num_scalar_prefetch=1,
            grid=(3,),
            in_specs=[block, block],
            out_specs=pl.BlockSpec((2 * Q, 512), lambda b, c: (0, b)),
        ),
        out_shape=jax.ShapeDtypeStruct((2 * Q, H), BF),
        name="turn_back",
    )(core, gate_mat, up_mat)


def weight_grads_kernel(x_ref, g1_ref, u1_ref, g2_ref, u2_ref, gate_ref, up_ref, norm_ref, turned_ref):
    @pl.when(pl.program_id(0) == 0)
    def _():
        for at, one_ref, two_ref in ((0, g1_ref, g2_ref), (384, u1_ref, u2_ref)):
            turned_ref[at : at + 384, 0:F1] = one_ref[...].T
            turned_ref[at : at + 384, F1:1152] = two_ref[...].T

    total = dot(turned_ref[...], x_ref[...])
    for k, ref in enumerate((gate_ref, up_ref)):
        part = total[384 * k : 384 * k + 384]
        norm_ref[k : k + 1, :] = jnp.sum(part * part, axis=0, keepdims=True)
        ref[...] = part.T.astype(BF)


def weight_grads(rows, g1, u1, g2, u2):
    def whole(a):
        return pl.BlockSpec(a.shape, lambda b: (0, 0))

    block = pl.BlockSpec((512, 384), lambda b: (b, 0))
    shape = jax.ShapeDtypeStruct((2 * H, 384), BF)
    return pl.pallas_call(
        weight_grads_kernel,
        grid=(6,),
        in_specs=[pl.BlockSpec((1152, 512), lambda b: (0, b)), whole(g1), whole(u1), whole(g2), whole(u2)],
        out_specs=[block, block, pl.BlockSpec((2, 512), lambda b: (0, b))],
        out_shape=[shape, shape, jax.ShapeDtypeStruct((2, 2 * H), F32)],
        scratch_shapes=[pltpu.VMEM((768, 1152), BF)],
        name="weight_grads",
    )(rows, g1, u1, g2, u2)


def to_experts(x):
    return lax.all_to_all(x, "ep", split_axis=0, concat_axis=0, tiled=True)


def swap_cores(x):
    return lax.ppermute(x, "tp", [(0, 1), (1, 0)])


def half(mat, index, axis):
    return lax.dynamic_slice_in_dim(mat, index * H, H, axis)


def step(tokens, cotangent, experts, gate, w_gate, w_up, w_down):
    core = lax.axis_index("tp").astype(jnp.int32)
    core_arg = core.reshape(1)
    gate_mat, up_mat, down_mat = w_gate[0], w_up[0], w_down[0]
    exp_t, gate_t = experts.T, gate.T
    gate_half, up_half = half(gate_mat, core, 0), half(up_mat, core, 0)
    down_turned = turn(down_mat)
    back_turned = turn_back(core_arg, gate_mat, up_mat)
    own, ranks, gates_of, lines = send_first(exp_t, gate_t, tokens, cotangent)
    own = to_experts(own)
    cot_two = send(ranks, gates_of, cotangent, 4, 9)
    by_token = token_ranks(experts)
    cot_two = to_experts(cot_two)
    other = swap_cores(own)

    rows_in, *terms = forward(core_arg, own, other, gate_mat, up_mat)

    def kept(gate_grad_pre, up_grad_pre):
        return (dot_last(gate_grad_pre, gate_half) + dot_last(up_grad_pre, up_half)).astype(BF)

    rows_one, gate_one, up_one, parts_one, sent = middle(
        core_arg, own, other, down_turned, back_turned, *terms, 0, False
    )
    sent = swap_cores(sent)
    back_one = kept(gate_one, up_one).astype(F32) + sent.astype(F32)
    back_one = back_one.astype(BF).reshape(E, 8, H)
    back_one = to_experts(back_one)

    cot_two_other = swap_cores(cot_two)
    rows_two, gate_two, up_two, parts_two, sent = middle(
        core_arg, cot_two, cot_two_other, down_turned, back_turned, *terms, 4, True
    )
    sent = swap_cores(sent)
    mine = kept(gate_two, up_two)
    parts = jnp.concatenate([parts_one, parts_two], axis=1)
    back_two = pack(mine, sent, parts, swap_cores(parts))
    back_two = to_experts(back_two)

    gate_grad, up_grad, norms = weight_grads(rows_in, gate_one, up_one, gate_two, up_two)
    norms = norms + swap_cores(norms)
    down_grad, down_norms = down_grads(terms[0], rows_one, rows_two)
    back_sum = combine_one(by_token, back_one)
    token_grad, gates_grad = combine_two(by_token, lines, exp_t, gate_t, back_sum, back_two)
    return (
        token_grad,
        gates_grad.T,
        gate_grad[None],
        up_grad[None],
        down_grad[None],
        norms[0:1],
        norms[1:2],
        down_norms,
    )


def solution(mesh):
    placed = (
        P("ep", "tp"),
        P("ep", "tp"),
        P("ep", None),
        P("ep", None),
        P("ep", None, "tp"),
        P("ep", None, "tp"),
        P("ep", "tp", None),
    )
    return jax.shard_map(
        step,
        mesh=mesh,
        in_specs=placed,
        out_specs=(
            P("ep", "tp"),
            P("ep", None),
            P("ep", None, "tp"),
            P("ep", None, "tp"),
            P("ep", "tp", None),
            P("ep", None),
            P("ep", None),
            P("ep", "tp"),
        ),
        check_vma=False,
    )
```

```python
import functools

import jax
import jax.numpy as jnp
from jax import lax
from jax.experimental import pallas as pl
from jax.experimental.pallas import tpu as pltpu
from jax.sharding import PartitionSpec as P


E = 64
TOK = 384
H = 1536
Q = 384
F1 = E * 8
BF = jnp.bfloat16
F32 = jnp.float32


def iota(shape, axis):
    return lax.broadcasted_iota(jnp.int32, shape, axis)


def dot(a, b):
    return lax.dot_general(a, b, (((1,), (0,)), ((), ())), preferred_element_type=F32)


def dot_last(a, b):
    return lax.dot_general(a, b, (((1,), (1,)), ((), ())), preferred_element_type=F32)


def dot_rows(a, b):
    return lax.dot_general(a, b, (((0,), (0,)), ((), ())), preferred_element_type=F32)


def ones_where(mask):
    return jnp.where(mask, 1.0, 0.0)


def named_by(exp):
    ids = iota((E, TOK), 0)
    return exp[0:1, :] == ids, exp[1:2, :] == ids


def slot_ranks(exp):
    first, second = named_by(exp)
    named = ones_where(first) + ones_where(second)
    earlier = ones_where(iota((TOK, TOK), 0) < iota((TOK, TOK), 1)).astype(BF)
    return named, dot(named.astype(BF), earlier)


def spread_rows(per_expert):
    spread = ones_where(iota((F1, E), 0) // 8 == iota((F1, E), 1)).astype(BF)
    return dot(spread, per_expert)


def row_slots(piece):
    i = iota((F1, TOK), 0) % 8
    return jnp.where(piece == 2, 16 + i % 2, i + 8 * piece).astype(F32)


def put_last(rows):
    row = iota((F1, 128), 0)
    col = iota((F1, 128), 1)
    total = jnp.zeros((F1, Q), F32)
    for q in range(4):
        place = ones_where(row == col // 2 * 8 + 2 * q + col % 2).astype(BF)
        total = total + dot(place, rows[:, q * Q : (q + 1) * Q])
    return total


def send_first_kernel(exp_ref, gate_ref, tok_ref, cot_ref, out_ref, ranks_ref, gates_ref, line_ref, small_ref):
    b = pl.program_id(0)

    @pl.when(b == 0)
    def _():
        exp = exp_ref[...]
        first, second = named_by(exp)
        named, ranks = slot_ranks(exp)
        small = jnp.where(named > 0.5, ranks, -1.0).astype(BF)
        small_ref[...] = small
        ranks_ref[...] = spread_rows(small)
        for k, mask in enumerate((first, second)):
            line_ref[k : k + 1, :] = jnp.sum(jnp.where(mask, ranks, 0.0), axis=0, keepdims=True)
        gate = gate_ref[...]
        rest = jnp.where(first, gate[0:1, :], 0.0) + jnp.where(second, gate[1:2, :], 0.0)
        total = jnp.zeros((F1, TOK), F32)
        for _ in range(3):
            part = rest.astype(BF)
            rest = rest - part.astype(F32)
            total = total + spread_rows(part)
        gates_ref[...] = total

    def rows(piece, lo, hi):
        hit = ones_where(ranks_ref[...] == row_slots(jnp.int32(piece))).astype(BF)
        return dot(hit, tok_ref[:, lo:hi]).reshape(E, 8, hi - lo).astype(BF)

    @pl.when(b == 0)
    def _():
        hit = ranks_ref[...] == row_slots(jnp.int32(0))
        scale = jnp.sum(jnp.where(hit, gates_ref[...], 0.0), axis=1, keepdims=True)
        scaled = dot(ones_where(hit).astype(BF), cot_ref[...]) * scale
        out_ref[:, :, 0:H] = scaled.reshape(E, 8, H).astype(BF)
        out_ref[:, :, H:1664] = rows(0, 0, 128)

    @pl.when(b == 1)
    def _():
        out_ref[:, :, 0:1408] = rows(0, 128, H)
        out_ref[:, :, 1408:1664] = rows(1, 0, 256)

    @pl.when(b == 2)
    def _():
        out_ref[:, :, 0:1280] = rows(1, 256, H)
        row = iota((128, E), 0)
        spread = ones_where(row // 2 == iota((128, E), 1)).astype(BF)
        slot = (16 + iota((128, TOK), 0) % 2).astype(F32)
        hit = ones_where(dot(spread, small_ref[...]) == slot).astype(BF)
        last = dot(hit, tok_ref[...]).astype(BF)
        out_ref[:, :, 1280:1664] = put_last(last).reshape(E, 8, Q).astype(BF)


def send_first(exp_t, gate_t, tokens, cotangent):
    small = pl.BlockSpec((2, TOK), lambda b: (0, 0))
    table = pl.BlockSpec((F1, TOK), lambda b: (0, 0))
    source = pl.BlockSpec((TOK, H), lambda b: (0, 0))
    shape = jax.ShapeDtypeStruct((F1, TOK), F32)
    return pl.pallas_call(
        send_first_kernel,
        grid=(3,),
        in_specs=[small, small, source, source],
        out_specs=[pl.BlockSpec((E, 8, 1664), lambda b: (0, 0, b)), table, table, small],
        out_shape=[
            jax.ShapeDtypeStruct((E, 8, 4992), BF),
            shape,
            shape,
            jax.ShapeDtypeStruct((2, TOK), F32),
        ],
        scratch_shapes=[pltpu.VMEM((E, TOK), BF)],
        name="send_first",
    )(exp_t, gate_t, tokens, cotangent)


def send_kernel(lo, last, ranks_ref, gates_ref, src_ref, out_ref):
    b = pl.program_id(0) + lo

    def scaled(hit, rows):
        rows = rows * jnp.sum(jnp.where(hit, gates_ref[...], 0.0), axis=1, keepdims=True)
        return rows.reshape(E, 8, Q).astype(BF)

    @pl.when(b < 8)
    def _():
        hit = ranks_ref[...] == row_slots(b // 4)
        src = src_ref[:, pl.ds(pl.multiple_of((b % 4) * Q, Q), Q)]
        out_ref[...] = scaled(hit, dot(ones_where(hit).astype(BF), src))

    if last:

        @pl.when(b == 8)
        def _():
            hit = ranks_ref[...] == row_slots(jnp.int32(2))
            block = (iota((F1, TOK), 0) % 8) // 2
            total = jnp.zeros((F1, Q), F32)
            for q in range(4):
                pick = ones_where(hit & (block == q)).astype(BF)
                total = total + dot(pick, src_ref[:, q * Q : (q + 1) * Q])
            out_ref[...] = scaled(hit, total)


def send(ranks, gates, src, lo, hi):
    whole = pl.BlockSpec((F1, TOK), lambda b: (0, 0))
    return pl.pallas_call(
        functools.partial(send_kernel, lo, hi == 9),
        grid=(hi - lo,),
        in_specs=[whole, whole, pl.BlockSpec((TOK, H), lambda b: (0, 0))],
        out_specs=pl.BlockSpec((E, 8, Q), lambda b: (0, 0, b)),
        out_shape=jax.ShapeDtypeStruct((E, 8, (hi - lo) * Q), BF),
        name="send",
    )(ranks, gates, src)


def unpack_last(last):
    flat = last.astype(F32).reshape(F1, Q).astype(BF)
    row = iota((128, F1), 0)
    pieces = []
    for q in range(4):
        pick = ones_where(row // 2 * 8 + 2 * q + row % 2 == iota((128, F1), 1)).astype(BF)
        pieces.append(dot(pick, flat).astype(BF))
    return pieces


def fill_rows(steps, core_ref, parts, rows_ref):
    b = pl.program_id(0)
    core = core_ref[0]
    halves = (core, 1 - core)

    @pl.when(b < steps)
    def _():
        for half, part_ref in zip(halves, parts[:2]):
            rows = part_ref[...].astype(F32).reshape(128, H).astype(BF)
            rows_ref[:, pl.ds(pl.multiple_of(half * H, H), H)] = rows

    if len(parts) == 4:

        @pl.when(b == steps)
        def _():
            for half, last_ref in zip(halves, parts[2:]):
                for q, piece in enumerate(unpack_last(last_ref[...])):
                    rows_ref[:, pl.ds(pl.multiple_of(half * H + q * Q, Q), Q)] = piece


def packed_specs(start, wide, last_at):
    steps = 4 * wide

    def rows_at(b):
        bb = jnp.minimum(b, steps - 1)
        return (bb % 4, 0, start + bb // 4)

    rows = pl.BlockSpec((16, 8, H), rows_at)
    last = pl.BlockSpec((E, 8, Q), lambda b: (0, 0, last_at))
    specs = [pl.BlockSpec(memory_space=pltpu.SMEM), rows, rows]
    return specs + [last, last] if last_at else specs


def forward_kernel(core_ref, own_ref, other_ref, own_last_ref, other_last_ref, *refs):
    gate_ref, up_ref, rows_ref, hidden_ref, active_ref, slope_ref = refs
    fill_rows(8, core_ref, (own_ref, other_ref, own_last_ref, other_last_ref), rows_ref)
    rows = rows_ref[...]
    gate_pre = dot(rows, gate_ref[...])
    up_pre = dot(rows, up_ref[...])
    sigma = jax.nn.sigmoid(gate_pre)
    active = gate_pre * sigma
    active_ref[...] = active.astype(BF)
    hidden_ref[...] = (active * up_pre).astype(BF)
    slope_ref[...] = (up_pre * sigma * (1.0 + gate_pre * (1.0 - sigma))).astype(BF)


def forward(core, own, other, gate_mat, up_mat):
    weights = pl.BlockSpec((2 * H, Q), lambda b: (0, 0))
    block = pl.BlockSpec((128, Q), lambda b: (b, 0))
    return pl.pallas_call(
        forward_kernel,
        grid=(9,),
        in_specs=packed_specs(1, 2, 12) + [weights, weights],
        out_specs=[pl.BlockSpec((128, 2 * H), lambda b: (b, 0)), block, block, block],
        out_shape=[
            jax.ShapeDtypeStruct((1152, 2 * H), BF),
            jax.ShapeDtypeStruct((1152, Q), BF),
            jax.ShapeDtypeStruct((1152, Q), BF),
            jax.ShapeDtypeStruct((1152, Q), BF),
        ],
        name="forward",
    )(core, own, other, own, other, gate_mat, up_mat)


def middle_kernel(core_ref, *refs):
    down_ref, back_ref, hidden_ref, active_ref, slope_ref = refs[-10:-5]
    rows_ref, gate_ref, up_ref, part_ref, sent_ref = refs[-5:]
    fill_rows(4, core_ref, refs[:-10], rows_ref)
    grad = dot(rows_ref[...], down_ref[...])
    part = jnp.sum(hidden_ref[...].astype(F32) * grad, axis=1, keepdims=True)
    part_ref[...] = jnp.broadcast_to(part, (128, 128)).T[0:1, :]
    gate = (grad * slope_ref[...].astype(F32)).astype(BF)
    up = (grad * active_ref[...].astype(F32)).astype(BF)
    gate_ref[...] = gate
    up_ref[...] = up
    sent_ref[...] = dot(jnp.concatenate([gate, up], axis=1), back_ref[...]).astype(BF)


def middle(core, own, other, down_turned, back_turned, hidden, active, slope, lo, last):
    taken = pl.BlockSpec((128, Q), lambda b: (b + lo, 0))
    block = pl.BlockSpec((128, Q), lambda b: (b, 0))
    steps = 5 if last else 4
    shape = jax.ShapeDtypeStruct((128 * steps, Q), BF)
    sides = (own, other, own, other) if last else (own, other)
    return pl.pallas_call(
        middle_kernel,
        grid=(steps,),
        in_specs=packed_specs(0, 1, 4 if last else 0)
        + [
            pl.BlockSpec((2 * H, Q), lambda b: (0, 0)),
            pl.BlockSpec((2 * Q, H), lambda b: (0, 0)),
            taken,
            taken,
            taken,
        ],
        out_specs=[
            pl.BlockSpec((128, 2 * H), lambda b: (b, 0)),
            block,
            block,
            pl.BlockSpec((1, 128), lambda b: (0, b)),
            pl.BlockSpec((128, H), lambda b: (b, 0)),
        ],
        out_shape=[
            jax.ShapeDtypeStruct((128 * steps, 2 * H), BF),
            shape,
            shape,
            jax.ShapeDtypeStruct((1, 128 * steps), F32),
            jax.ShapeDtypeStruct((128 * steps, H), BF),
        ],
        name="middle",
    )(core, *sides, down_turned, back_turned, hidden, active, slope)


def pack_kernel(mine_ref, got_ref, mine_last_ref, got_last_ref, part_ref, got_part_ref, out_ref):
    b = pl.program_id(0)

    @pl.when(b < 3)
    def _():
        total = mine_ref[...].astype(F32) + got_ref[...].astype(F32)
        out_ref[...] = total.reshape(E, 8, 512).astype(BF)

    @pl.when(b == 3)
    def _():
        total = (mine_last_ref[...].astype(F32) + got_last_ref[...].astype(F32)).astype(BF)
        out_ref[:, :, 0:Q] = put_last(total).reshape(E, 8, Q).astype(BF)
        products = (part_ref[...] + got_part_ref[...]).astype(BF).astype(F32)
        at = iota((E, 1152), 1)
        source = jnp.where(at < 1024, at % 512 // 8, (at - 1024) // 2)
        mine = jnp.where(source == iota((E, 1152), 0), products, 0.0).astype(BF)
        at = iota((1152, 128), 0)
        slot = jnp.where(at < 1024, at // 512 * 8 + at % 8, 16 + at % 2)
        table = dot(mine, ones_where(slot == iota((1152, 128), 1)).astype(BF)).astype(BF)
        place = ones_where(iota((F1, E), 0) == 8 * iota((F1, E), 1)).astype(BF)
        out_ref[:, :, Q:512] = dot(place, table).reshape(E, 8, 128).astype(BF)


def pack(mine, got, part, got_part):
    main = pl.BlockSpec((F1, 512), lambda b: (0, jnp.minimum(b, 2)))
    last = pl.BlockSpec((128, H), lambda b: (4, 0))
    line = pl.BlockSpec((1, 1152), lambda b: (0, 0))
    return pl.pallas_call(
        pack_kernel,
        grid=(4,),
        in_specs=[main, main, last, last, line, line],
        out_specs=pl.BlockSpec((E, 8, 512), lambda b: (0, 0, b)),
        out_shape=jax.ShapeDtypeStruct((E, 8, 2048), BF),
        name="pack",
    )(mine, got, mine, got, part, got_part)


def token_ranks_kernel(exp_ref, out_ref):
    exp = exp_ref[...]
    ids = iota((TOK, E), 1)
    named = ones_where(exp[:, 0:1] == ids) + ones_where(exp[:, 1:2] == ids)
    earlier = ones_where(iota((TOK, TOK), 1) < iota((TOK, TOK), 0)).astype(BF)
    ranks = jnp.where(named > 0.5, dot(earlier, named.astype(BF)), -1.0).astype(BF)
    spread = ones_where(iota((E, F1), 0) == iota((E, F1), 1) // 8).astype(BF)
    out_ref[...] = dot(ranks, spread)


def token_ranks(experts):
    return pl.pallas_call(
        token_ranks_kernel, out_shape=jax.ShapeDtypeStruct((TOK, F1), F32), name="token_ranks"
    )(experts)


def flat_rows(ref):
    return ref[...].astype(F32).reshape(F1, ref.shape[2]).astype(BF)


def column_slots(piece):
    i = iota((TOK, F1), 1) % 8
    return (16 + i % 2 if piece == 2 else i + 8 * piece).astype(F32)


def combine_one_kernel(ranks_ref, one_ref, out_ref):
    hit = ones_where(ranks_ref[...] == column_slots(0)).astype(BF)
    out_ref[...] = dot(hit, flat_rows(one_ref))


def combine_one(ranks, one):
    return pl.pallas_call(
        combine_one_kernel,
        grid=(2,),
        in_specs=[
            pl.BlockSpec((TOK, F1), lambda b: (0, 0)),
            pl.BlockSpec((E, 8, 2 * Q), lambda b: (0, 0, b)),
        ],
        out_specs=pl.BlockSpec((TOK, 2 * Q), lambda b: (0, b)),
        out_shape=jax.ShapeDtypeStruct((TOK, H), F32),
        name="combine_one",
    )(ranks, one)


def combine_two_kernel(ranks_ref, line_ref, exp_ref, gate_ref, *refs):
    sum_ref, two_ref, last_ref, prod_ref, out_ref, gate_out_ref = refs
    b = pl.program_id(0)

    @pl.when(b == 0)
    def _():
        pick = ones_where(iota((E, F1), 1) == 8 * iota((E, F1), 0)).astype(BF)
        table = dot(pick, flat_rows(prod_ref)).astype(BF)
        for k in range(2):
            named = ones_where(iota((E, TOK), 0) == exp_ref[k : k + 1, :]).astype(BF)
            found = dot_rows(table, named)
            here = iota((128, TOK), 0).astype(F32) == line_ref[k : k + 1, :]
            found = jnp.sum(jnp.where(here, found, 0.0), axis=0, keepdims=True)
            gate_out_ref[k : k + 1, :] = found / gate_ref[k : k + 1, :]

    ranks = ranks_ref[...]
    block = iota((TOK, F1), 1) % 8 // 2
    total = sum_ref[...] + dot(ones_where(ranks == column_slots(1)).astype(BF), flat_rows(two_ref))
    last = flat_rows(last_ref)
    for j in range(2):
        hit = (ranks == column_slots(2)) & (block == 2 * b + j)
        part = total[:, j * Q : (j + 1) * Q] + dot(ones_where(hit).astype(BF), last)
        out_ref[:, j * Q : (j + 1) * Q] = part.astype(BF)


def combine_two(ranks, lines, exp_t, gate_t, total, two):
    small = pl.BlockSpec((2, TOK), lambda b: (0, 0))
    return pl.pallas_call(
        combine_two_kernel,
        grid=(2,),
        in_specs=[
            pl.BlockSpec((TOK, F1), lambda b: (0, 0)),
            small,
            small,
            small,
            pl.BlockSpec((TOK, 2 * Q), lambda b: (0, b)),
            pl.BlockSpec((E, 8, 2 * Q), lambda b: (0, 0, b)),
            pl.BlockSpec((E, 8, Q), lambda b: (0, 0, 4)),
            pl.BlockSpec((E, 8, 128), lambda b: (0, 0, 15)),
        ],
        out_specs=[pl.BlockSpec((TOK, 2 * Q), lambda b: (0, b)), small],
        out_shape=[jax.ShapeDtypeStruct((TOK, H), BF), jax.ShapeDtypeStruct((2, TOK), F32)],
        name="combine_two",
    )(ranks, lines, exp_t, gate_t, total, two, two, two)


def down_grads_kernel(hidden_ref, one_ref, two_ref, out_ref, norm_ref, turned_ref, sums_ref):
    b = pl.program_id(0)

    @pl.when(b == 0)
    def _():
        turned_ref[...] = hidden_ref[...].T
        sums_ref[...] = jnp.zeros((Q, 128), F32)

    total = dot(turned_ref[:, 0:F1], one_ref[...]) + dot(turned_ref[:, F1:1152], two_ref[...])
    out_ref[...] = total.astype(BF)
    sums_ref[...] += jnp.broadcast_to(jnp.sum(total * total, axis=1, keepdims=True), (Q, 128))

    @pl.when(b == 5)
    def _():
        norm_ref[...] = sums_ref[...].T[0:1, :]


def down_grads(hidden, one, two):
    return pl.pallas_call(
        down_grads_kernel,
        grid=(6,),
        in_specs=[
            pl.BlockSpec((1152, Q), lambda b: (0, 0)),
            pl.BlockSpec((F1, 512), lambda b: (0, b)),
            pl.BlockSpec((640, 512), lambda b: (0, b)),
        ],
        out_specs=[pl.BlockSpec((Q, 512), lambda b: (0, b)), pl.BlockSpec((1, Q), lambda b: (0, 0))],
        out_shape=[jax.ShapeDtypeStruct((Q, 2 * H), BF), jax.ShapeDtypeStruct((1, Q), F32)],
        scratch_shapes=[pltpu.VMEM((Q, 1152), BF), pltpu.VMEM((Q, 128), F32)],
        name="down_grads",
    )(hidden, one, two)


def turn_kernel(src_ref, out_ref):
    out_ref[...] = src_ref[...].T


def turn(mat):
    return pl.pallas_call(
        turn_kernel,
        grid=(6,),
        in_specs=[pl.BlockSpec((Q, 512), lambda b: (0, b))],
        out_specs=pl.BlockSpec((512, Q), lambda b: (b, 0)),
        out_shape=jax.ShapeDtypeStruct((2 * H, Q), BF),
        name="turn",
    )(mat)


def turn_back_kernel(core_ref, gate_ref, up_ref, out_ref):
    out_ref[0:Q, :] = gate_ref[...].T
    out_ref[Q : 2 * Q, :] = up_ref[...].T


def turn_back(core, gate_mat, up_mat):
    block = pl.BlockSpec((512, Q), lambda b, c: (3 * (1 - c[0]) + b, 0))
    return pl.pallas_call(
        turn_back_kernel,
        grid_spec=pltpu.PrefetchScalarGridSpec(
            num_scalar_prefetch=1,
            grid=(3,),
            in_specs=[block, block],
            out_specs=pl.BlockSpec((2 * Q, 512), lambda b, c: (0, b)),
        ),
        out_shape=jax.ShapeDtypeStruct((2 * Q, H), BF),
        name="turn_back",
    )(core, gate_mat, up_mat)


def weight_grads_kernel(x_ref, g1_ref, u1_ref, g2_ref, u2_ref, gate_ref, up_ref, norm_ref, turned_ref):
    @pl.when(pl.program_id(0) == 0)
    def _():
        for at, one_ref, two_ref in ((0, g1_ref, g2_ref), (384, u1_ref, u2_ref)):
            turned_ref[at : at + 384, 0:F1] = one_ref[...].T
            turned_ref[at : at + 384, F1:1152] = two_ref[...].T

    total = dot(turned_ref[...], x_ref[...])
    for k, ref in enumerate((gate_ref, up_ref)):
        part = total[384 * k : 384 * k + 384]
        norm_ref[k : k + 1, :] = jnp.sum(part * part, axis=0, keepdims=True)
        ref[...] = part.T.astype(BF)


def weight_grads(rows, g1, u1, g2, u2):
    def whole(a):
        return pl.BlockSpec(a.shape, lambda b: (0, 0))

    block = pl.BlockSpec((512, 384), lambda b: (b, 0))
    shape = jax.ShapeDtypeStruct((2 * H, 384), BF)
    return pl.pallas_call(
        weight_grads_kernel,
        grid=(6,),
        in_specs=[pl.BlockSpec((1152, 512), lambda b: (0, b)), whole(g1), whole(u1), whole(g2), whole(u2)],
        out_specs=[block, block, pl.BlockSpec((2, 512), lambda b: (0, b))],
        out_shape=[shape, shape, jax.ShapeDtypeStruct((2, 2 * H), F32)],
        scratch_shapes=[pltpu.VMEM((768, 1152), BF)],
        name="weight_grads",
    )(rows, g1, u1, g2, u2)


def to_experts(x):
    return lax.all_to_all(x, "ep", split_axis=0, concat_axis=0, tiled=True)


def swap_cores(x):
    return lax.ppermute(x, "tp", [(0, 1), (1, 0)])


def half(mat, index, axis):
    return lax.dynamic_slice_in_dim(mat, index * H, H, axis)


def step(tokens, cotangent, experts, gate, w_gate, w_up, w_down):
    core = lax.axis_index("tp").astype(jnp.int32)
    core_arg = core.reshape(1)
    gate_mat, up_mat, down_mat = w_gate[0], w_up[0], w_down[0]
    exp_t, gate_t = experts.T, gate.T
    gate_half, up_half = half(gate_mat, core, 0), half(up_mat, core, 0)
    down_turned = turn(down_mat)
    back_turned = turn_back(core_arg, gate_mat, up_mat)
    own, ranks, gates_of, lines = send_first(exp_t, gate_t, tokens, cotangent)
    own = to_experts(own)
    cot_two = send(ranks, gates_of, cotangent, 4, 9)
    by_token = token_ranks(experts)
    cot_two = to_experts(cot_two)
    other = swap_cores(own)

    rows_in, *terms = forward(core_arg, own, other, gate_mat, up_mat)

    def kept(gate_grad_pre, up_grad_pre):
        return (dot_last(gate_grad_pre, gate_half) + dot_last(up_grad_pre, up_half)).astype(BF)

    rows_one, gate_one, up_one, parts_one, sent = middle(
        core_arg, own, other, down_turned, back_turned, *terms, 0, False
    )
    sent = swap_cores(sent)
    back_one = kept(gate_one, up_one).astype(F32) + sent.astype(F32)
    back_one = back_one.astype(BF).reshape(E, 8, H)
    back_one = to_experts(back_one)

    cot_two_other = swap_cores(cot_two)
    rows_two, gate_two, up_two, parts_two, sent = middle(
        core_arg, cot_two, cot_two_other, down_turned, back_turned, *terms, 4, True
    )
    sent = swap_cores(sent)
    mine = kept(gate_two, up_two)
    parts = jnp.concatenate([parts_one, parts_two], axis=1)
    back_two = pack(mine, sent, parts, swap_cores(parts))
    back_two = to_experts(back_two)

    gate_grad, up_grad, norms = weight_grads(rows_in, gate_one, up_one, gate_two, up_two)
    norms = norms + swap_cores(norms)
    down_grad, down_norms = down_grads(terms[0], rows_one, rows_two)
    back_sum = combine_one(by_token, back_one)
    token_grad, gates_grad = combine_two(by_token, lines, exp_t, gate_t, back_sum, back_two)
    return (
        token_grad,
        gates_grad.T,
        gate_grad[None],
        up_grad[None],
        down_grad[None],
        norms[0:1],
        norms[1:2],
        down_norms,
    )


def solution(mesh):
    placed = (
        P("ep", "tp"),
        P("ep", "tp"),
        P("ep", None),
        P("ep", None),
        P("ep", None, "tp"),
        P("ep", None, "tp"),
        P("ep", "tp", None),
    )
    return jax.shard_map(
        step,
        mesh=mesh,
        in_specs=placed,
        out_specs=(
            P("ep", "tp"),
            P("ep", None),
            P("ep", None, "tp"),
            P("ep", None, "tp"),
            P("ep", "tp", None),
            P("ep", None),
            P("ep", None),
            P("ep", "tp"),
        ),
        check_vma=False,
    )
```
